32 devices in a mesh: grp: 2 (over x), ep: 16 (over z, y, core).
Axes of the slice: x: 2, y: 2, z: 4, core: 2. Of those that a mesh axis runs over, the one named last changes fastest.
Arguments:
- hidden: bfloat16 [4096, 2048], P(('grp', 'ep')), parts along dimension 0, may hold values from -6 to 6
- state: float32 [2, 4096, 4096], P(None, ('grp', 'ep')), parts along dimension 1, may hold values from -6 to 6
- norm_gain: float32 [2048], replicated, may hold values from 0.1 to 1.9
- w_in: bfloat16 [2048, 1024], P(None, 'ep'), may hold values from -0.125 to 0.125
- lam_re: float32 [64, 64], replicated, may hold values from -1 to -0.1
- lam_im: float32 [64, 64], replicated, may hold values from 0 to 200
- log_step: float32 [64], replicated, may hold values from -4.6 to -0.7
- in_re: float32 [64, 64, 16], replicated, may hold values from -1 to 1
- in_im: float32 [64, 64, 16], replicated, may hold values from -1 to 1
- out_re: float32 [64, 16, 64], replicated, may hold values from -0.75 to 0.75
- out_im: float32 [64, 16, 64], replicated, may hold values from -0.75 to 0.75
- skip: float32 [1024], replicated, may hold values from -4 to 4
- w_glu: bfloat16 [1024, 1024], replicated, may hold values from -0.1875 to 0.1875
- w_out: bfloat16 [1024, 2048], replicated, may hold values from -0.375 to 0.375
- ffn_gain: float32 [2048], replicated, may hold values from 0.1 to 1.9
- w_group: bfloat16 [2048, 4], replicated, may hold values from -0.03125 to 0.03125
- w_route: bfloat16 [2048, 16], replicated, may hold values from -0.03125 to 0.03125
- w_gate: bfloat16 [16, 2048, 512], P('ep'), may hold values from -0.125 to 0.125
- w_up: bfloat16 [16, 2048, 512], P('ep'), may hold values from -0.125 to 0.125
- w_down: bfloat16 [16, 512, 2048], P('ep'), may hold values from -2 to 2
- route_ids: int32 [4096, 2], P(('grp', 'ep')), parts along dimension 0, may hold values from 0 to 15, as said below
Outputs:
- hidden_out: bfloat16 [4096, 2048], P(('grp', 'ep')), parts along dimension 0
- new_state: float32 [2, 4096, 4096], P(None, ('grp', 'ep')), parts along dimension 1
The draws below stay inside these ranges and needn't reach their ends.
There are 2 independent parts, one for each index of `grp`. The reference program is written for one: setup_inputs(seed, part) draws one part's arguments, and reference() takes and returns one part's arrays. A program takes and returns all parts, laid end to end along the dimension named above; an argument that names none is the same for every part. Nothing has to cross between parts.
Inputs may be any that keep to these rules, and one draw needn't show every extreme that they name: `route_ids`: each row names 2 different experts of one expert group (experts g * 4 to g * 4 + 3). Among the rows of one device no expert is named more than 32 times, and in every draw some experts are named exactly 32 times by the rows of every device.
All inputs are finite; a program needn't handle non-finite values.
Results may differ from the reference program's by a relative error of at most 0.013.
Values may be sent and summed in bfloat16 or wider, within the bound.
A program may use at most 128 MiB of HBM per device.

```python
import jax
import jax.numpy as jnp
from jax import lax

D = 2048
S5W = 1024
GROUP_CH = 16
STATE = 64
FFE = 512
EXP_GROUPS = 4
TOPK = 2
SEQ_DEV = 128
SEQS = 2048
EXPERTS = 16
EPG = 4
CAP = 32
GROUPS_S5 = 64
N_EP = 16


def draw_route_ids(key, part):
    base = jax.random.fold_in(key, 11)
    big_key, rest_key = jax.random.split(base)
    big = jax.random.randint(big_key, (), 0, EXP_GROUPS)
    half = SEQ_DEV // 2

    def one_block(block_key):
        order_key, other_key, shift_key, label_key = jax.random.split(block_key, 4)
        order = jax.random.permutation(order_key, SEQ_DEV)
        others = (big + 1 + jax.random.randint(other_key, (SEQ_DEV,), 0, EXP_GROUPS - 1)) % EXP_GROUPS
        by_place = jnp.where(jnp.arange(SEQ_DEV) < half, big, others).astype(jnp.int32)
        group = jnp.zeros((SEQ_DEV,), jnp.int32).at[order].set(by_place)
        member = (group[:, None] == jnp.arange(EXP_GROUPS, dtype=jnp.int32)[None, :]).astype(jnp.int32)
        rank = jnp.sum((jnp.cumsum(member, axis=0) - member) * member, axis=1)
        shift = jax.random.randint(shift_key, (EXP_GROUPS,), 0, EPG)
        labels = jax.vmap(lambda sub: jax.random.permutation(sub, EPG))(jax.random.split(label_key, EXP_GROUPS))
        first = (2 * rank + shift[group]) % EPG
        second = (2 * rank + 1 + shift[group]) % EPG
        one = group * EPG + labels[group, first]
        two = group * EPG + labels[group, second]
        return jnp.stack([one, two], axis=1).astype(jnp.int32)
    blocks = jax.vmap(one_block)(jax.random.split(rest_key, SEQS // SEQ_DEV))
    return blocks.reshape(SEQS, TOPK)


def block_scale(stream_key, extent, cuts, low, top_value):
    def one(axis_at, parts):
        draws = jax.random.uniform(jax.random.fold_in(jax.random.fold_in(stream_key, 6), axis_at), (parts,), jnp.float32, low / len(cuts), top_value / len(cuts))
        return jnp.repeat(jnp.exp(draws), extent[axis_at] // parts).reshape((-1,) + (1,) * (len(extent) - axis_at - 1))

    level = one(*cuts[0])
    for cut in cuts[1:]:
        level = level * one(*cut)
    return level


def gaussian(own_key, extent, scale, most, pieces=(), held_as=jnp.bfloat16):
    array = scale * jax.random.normal(own_key, extent, jnp.float32)
    if pieces:
        array = array * block_scale(own_key, extent, pieces, -0.22, 0.18)
    return jnp.clip(array, -most, most).astype(held_as)


def setup_inputs(seed: int = 0, part: int = 0) -> dict:
    key_list = jax.random.split(jax.random.key(seed), 22)
    own_keys = jax.random.split(jax.random.fold_in(key_list[21], part), 22)
    hidden = gaussian(own_keys[0], (SEQS, D), 1.0, 6.0, ((0, 16),))
    state = gaussian(own_keys[1], (2, SEQS, GROUPS_S5 * STATE), 1.0, 6.0, ((1, 16),), jnp.float32)
    norm_gain = jnp.clip(1.0 + 0.18 * jax.random.normal(key_list[2], (D,), jnp.float32), 0.1, 1.9)
    w_in = gaussian(key_list[3], (D, S5W), D ** -0.5, 0.125, ((1, 16),))
    lam_re = jnp.clip(jax.random.uniform(key_list[4], (GROUPS_S5, STATE), jnp.float32, -1.0, -0.1), -1.0, -0.1)
    lam_im = jnp.clip(jax.random.uniform(key_list[5], (GROUPS_S5, STATE), jnp.float32, 0.0, 200.0), 0.0, 200.0)
    log_step = jnp.clip(jax.random.uniform(key_list[6], (GROUPS_S5,), jnp.float32, -4.6, -0.7), -4.6, -0.7)
    in_re = gaussian(key_list[7], (GROUPS_S5, STATE, GROUP_CH), (2 * GROUP_CH) ** -0.5, 1.0, (), jnp.float32)
    in_im = gaussian(key_list[8], (GROUPS_S5, STATE, GROUP_CH), (2 * GROUP_CH) ** -0.5, 1.0, (), jnp.float32)
    out_re = gaussian(key_list[9], (GROUPS_S5, GROUP_CH, STATE), STATE ** -0.5, 0.75, (), jnp.float32)
    out_im = gaussian(key_list[10], (GROUPS_S5, GROUP_CH, STATE), STATE ** -0.5, 0.75, (), jnp.float32)
    skip = gaussian(key_list[11], (S5W,), 1.0, 4.0, (), jnp.float32)
    w_glu = gaussian(key_list[12], (S5W, S5W), S5W ** -0.5, 0.1875)
    w_out = gaussian(key_list[13], (S5W, D), (S5W // 4) ** -0.5, 0.375)
    ffn_gain = jnp.clip(1.0 + 0.18 * jax.random.normal(key_list[14], (D,), jnp.float32), 0.1, 1.9)
    w_group = gaussian(key_list[15], (D, EXP_GROUPS), (16 * D) ** -0.5, 0.03125)
    w_route = gaussian(key_list[16], (D, EXPERTS), (16 * D) ** -0.5, 0.03125)
    w_gate = gaussian(key_list[17], (EXPERTS, D, FFE), D ** -0.5, 0.125, ((0, 16),))
    w_up = gaussian(key_list[18], (EXPERTS, D, FFE), D ** -0.5, 0.125, ((0, 16),))
    w_down = gaussian(key_list[19], (EXPERTS, FFE, D), (max(FFE // 64, 1)) ** -0.5, 2.0, ((0, 16),))
    route_ids = draw_route_ids(jax.random.fold_in(jax.random.fold_in(key_list[21], part), 71), part)
    return dict(hidden=hidden, state=state, norm_gain=norm_gain, w_in=w_in, lam_re=lam_re, lam_im=lam_im, log_step=log_step, in_re=in_re, in_im=in_im, out_re=out_re, out_im=out_im, skip=skip, w_glu=w_glu, w_out=w_out, ffn_gain=ffn_gain, w_group=w_group, w_route=w_route, w_gate=w_gate, w_up=w_up, w_down=w_down, route_ids=route_ids)


def normalize(rows, gain):
    wide = rows.astype(jnp.float32)
    return wide * lax.rsqrt(lax.optimization_barrier(jnp.mean(wide * wide, axis=-1, keepdims=True)) + 1e-06) * gain

def discretize(lam_re, lam_im, log_step, in_re, in_im):
    step = jnp.exp(log_step)[:, None]
    magnitude = jnp.exp(lam_re * step)
    bar_re = magnitude * jnp.cos(lam_im * step)
    bar_im = magnitude * jnp.sin(lam_im * step)
    denom = lam_re * lam_re + lam_im * lam_im
    lessened = bar_re - 1.0
    coef_re = (lessened * lam_re + bar_im * lam_im) / denom
    coef_im = (bar_im * lam_re - lessened * lam_im) / denom
    drive_re = coef_re[:, :, None] * in_re - coef_im[:, :, None] * in_im
    drive_im = coef_re[:, :, None] * in_im + coef_im[:, :, None] * in_re
    return (bar_re, bar_im, drive_re, drive_im)

def mixer_step(inputs, state, lam_re, lam_im, log_step, in_re, in_im, out_re, out_im, skip, w_glu):
    rows = inputs.shape[0]
    groups, entries = lam_re.shape
    width = in_re.shape[2]
    highest = lax.Precision.HIGHEST
    bar_re, bar_im, drive_re, drive_im = discretize(lam_re, lam_im, log_step, in_re, in_im)
    wide = inputs.astype(jnp.float32)
    grouped = wide.reshape(rows, groups, width)
    push_re = jnp.einsum('bgc,gnc->bgn', grouped, drive_re, precision=highest)
    push_im = jnp.einsum('bgc,gnc->bgn', grouped, drive_im, precision=highest)
    old_re = state[0].reshape(rows, groups, entries)
    old_im = state[1].reshape(rows, groups, entries)
    new_re = bar_re * old_re - bar_im * old_im + push_re
    new_im = bar_re * old_im + bar_im * old_re + push_im
    read = jnp.einsum('bgn,gcn->bgc', new_re, out_re, precision=highest) - jnp.einsum('bgn,gcn->bgc', new_im, out_im, precision=highest)
    mixed = read.reshape(rows, groups * width) + skip * wide
    active = jax.nn.gelu(mixed)
    gating = jnp.dot(active.astype(jnp.bfloat16), w_glu, preferred_element_type=jnp.float32)
    result = (active * jax.nn.sigmoid(gating)).astype(jnp.bfloat16)
    new_state = jnp.stack([new_re.reshape(rows, -1), new_im.reshape(rows, -1)])
    return (result, new_state)

def route_gates(normed, w_group, w_route, route_ids, per_group):
    group_logit = jnp.dot(normed, w_group, preferred_element_type=jnp.float32)
    route_logit = jnp.dot(normed, w_route, preferred_element_type=jnp.float32)
    chosen = route_ids[:, 0] // per_group
    pick_group = (chosen[:, None] == jnp.arange(group_logit.shape[1], dtype=jnp.int32)[None, :]).astype(jnp.float32)
    own = lax.optimization_barrier(jnp.sum(group_logit * pick_group, axis=1, keepdims=True))
    group_weight = 1.0 / lax.optimization_barrier(jnp.sum(jnp.exp(group_logit - own), axis=1))
    pick = (route_ids[:, :, None] == jnp.arange(route_logit.shape[1], dtype=jnp.int32)[None, None, :]).astype(jnp.float32)
    chosen_logit = lax.optimization_barrier(jnp.sum(pick * route_logit[:, None, :], axis=2))
    first = jax.nn.sigmoid(chosen_logit[:, 0] - chosen_logit[:, 1])
    pair = jnp.stack([first, 1.0 - first], axis=1)
    return group_weight[:, None] * pair

def reference(hidden, state, norm_gain, w_in, lam_re, lam_im, log_step, in_re, in_im, out_re, out_im, skip, w_glu, w_out, ffn_gain, w_group, w_route, w_gate, w_up, w_down, route_ids):
    normed = normalize(hidden, norm_gain).astype(jnp.bfloat16)
    inputs = jnp.dot(normed, w_in, preferred_element_type=jnp.float32).astype(jnp.bfloat16)
    glu, new_state = mixer_step(inputs, state, lam_re, lam_im, log_step, in_re, in_im, out_re, out_im, skip, w_glu)
    resid = (hidden.astype(jnp.float32) + jnp.dot(glu, w_out, preferred_element_type=jnp.float32)).astype(jnp.bfloat16)
    normed2 = normalize(resid, ffn_gain).astype(jnp.bfloat16)
    gates = route_gates(normed2, w_group, w_route, route_ids, EPG)
    limit = N_EP * CAP

    def visit(total, expert):
        hit = route_ids == expert
        weight = lax.optimization_barrier(jnp.sum(jnp.where(hit, gates, 0.0), axis=1))
        used = jnp.any(hit, axis=1)
        count = jnp.sum(used.astype(jnp.int32))
        index = jnp.nonzero(used, size=limit, fill_value=0)[0].astype(jnp.int32)
        valid = (jnp.arange(limit, dtype=jnp.int32) < count).astype(jnp.float32)
        rows = normed2[index]
        gate = jnp.dot(rows, w_gate[expert], preferred_element_type=jnp.float32)
        upper = jnp.dot(rows, w_up[expert], preferred_element_type=jnp.float32)
        inner = (jax.nn.silu(gate) * upper).astype(jnp.bfloat16)
        result = jnp.dot(inner, w_down[expert], preferred_element_type=jnp.float32).astype(jnp.bfloat16)
        scale = weight[index] * valid
        total = total.at[index].add(scale[:, None] * result.astype(jnp.float32))
        return (total, None)
    start = jnp.zeros((hidden.shape[0], hidden.shape[1]), jnp.float32)
    total, unused = lax.scan(visit, start, jnp.arange(EXPERTS, dtype=jnp.int32))
    hidden_out = (resid.astype(jnp.float32) + total).astype(jnp.bfloat16)
    return (hidden_out, new_state)
```

```python
import functools

import jax
import jax.numpy as jnp
from jax import lax
from jax.experimental import pallas as pl
from jax.experimental.pallas import tpu as pltpu
from jax.sharding import PartitionSpec as P

EXP_GROUPS = 4
TOPK = 2
MESH = pl.DeviceIdType.MESH
VMEM = pl.BlockSpec(memory_space=pltpu.VMEM)
ANY = pl.BlockSpec(memory_space=pl.ANY)
F32 = jnp.float32
BF16 = jnp.bfloat16
NT = (((1,), (1,)), ((), ()))
TN = (((0,), (0,)), ((), ()))
LIMIT = 60 * 1024 * 1024
FRONT_LIMIT = 44 * 1024 * 1024


def remote(src, dst, send_sem, recv_sem, device):
    return pltpu.make_async_remote_copy(
        src_ref=src, dst_ref=dst, send_sem=send_sem, recv_sem=recv_sem, device_id=device, device_id_type=MESH
    )


def greet(peers):
    barrier = pltpu.get_barrier_semaphore()
    for peer in peers:
        pl.semaphore_signal(barrier, inc=1, device_id=peer, device_id_type=MESH)
    pl.semaphore_wait(barrier, len(peers))


def front_kernel(
    chips, per_group, hidden_any, gain_ref, w_any, state_any, lam_re_ref, lam_im_ref, step_ref, in_re_any, in_im_any,
    out_re_any, out_im_any, skip_ref, ffn_gain_ref, w_glu_any, w_out_any, w_group_ref, w_route_ref, ids_ref,
    new_any, resid_ref, rows_ref, place_ref,
    held, hidden, state, in_re, in_im, out_re, out_im, glu_w, out_w, normed, coef, active, gating,
    zs, zr, ys, yr, xs, xr, ds, dr, own_s, own_r, load_sems, state_sems, new_sems,
):
    grp = lax.axis_index("grp")
    me = lax.axis_index("ep")
    chip, core = me // 2, me % 2
    lines = chips // 2
    line, y = chip // 2, chip % 2
    side = grp % 2
    shard, depth = w_any.shape
    entries = lam_re_ref.shape[1]
    unit = 128 // (2 * shard)
    blocks = chips // unit
    span = state.shape[2] // blocks
    channels = 128 // (span // entries)

    def at(row, column):
        return (grp, (row * 2 + column) * 2 + core)

    mate = (grp, me + 1 - 2 * core)
    across = (grp + 1 - 2 * side, me)
    beside = at(line, 1 - y)
    after = lines - 1 - line
    longer = (after - line + lines - 1) // lines
    short = line * longer + after * (1 - longer)

    def near(k):
        past = (k + 2 * lines - 2 * short) // (2 * lines)
        paired = (k // 2 + 1) * (1 - 2 * (k % 2))
        single = (k - short + 1) * (2 * longer - 1)
        return line + paired * (1 - past) + single * past

    order = [near(k) for k in range(lines - 1)]
    third = depth // 3 // 128 * 128
    middle = depth - 2 * third
    cols = [
        pl.ds(pl.multiple_of(side * (depth - third), 128), third),
        pl.ds(third, middle),
        pl.ds(pl.multiple_of((1 - side) * (depth - third), 128), third),
    ]
    sends = []

    def start(copy):
        copy.start()
        sends.append(copy)

    def column(j):
        return pl.ds(pl.multiple_of(j * span, 128), span)

    own = pltpu.make_async_copy(w_any, held.at[chip, core], load_sems.at[0])
    own.start()
    loads = [
        pltpu.make_async_copy(src, dst, load_sems.at[1 + i])
        for i, (src, dst) in enumerate([
            (hidden_any, hidden), (in_re_any, in_re), (in_im_any, in_im), (out_re_any, out_re), (out_im_any, out_im),
            (w_glu_any, glu_w), (w_out_any, out_w),
        ])
    ]
    for load in loads[:1]:
        load.start()
    greet([at(o, y) for o in order] + [beside, mate, across])
    own.wait()
    for p in range(2):
        spot = held.at[chip, core, :, cols[p]]
        start(remote(spot, spot, ys.at[line, p], yr.at[line, p], beside))
        for o in order:
            start(remote(spot, spot, zs.at[o, p], zr.at[line, p], at(o, y)))
    spot = held.at[chip, core]
    start(remote(spot, spot, own_s, own_r, mate))
    for load in loads[1:]:
        load.start()
    block_loads = [
        pltpu.make_async_copy(state_any.at[:, :, pl.ds(j * span, span)], state.at[:, :, pl.ds(j * span, span)], state_sems.at[j])
        for j in range(blocks)
    ]
    for load in block_loads:
        load.start()

    def iota(shape, axis):
        return lax.broadcasted_iota(jnp.int32, shape, axis)

    loads[0].wait()
    wide = hidden[...].astype(F32)
    mean = jnp.mean(wide * wide, axis=-1, keepdims=True)
    normed[...] = (wide * lax.rsqrt(mean + 1e-06) * gain_ref[...]).astype(BF16)

    groups = lam_re_ref.shape[0]
    lr, li = lam_re_ref[...], lam_im_ref[...]
    diagonal = iota((groups, groups), 0) == iota((groups, groups), 1)
    step = jnp.exp(jnp.sum(jnp.where(diagonal, step_ref[...], 0.0), axis=1, keepdims=True))
    magnitude = jnp.exp(lr * step)
    bar_re = magnitude * jnp.cos(li * step)
    bar_im = magnitude * jnp.sin(li * step)
    denom = lr * lr + li * li
    lessened = bar_re - 1.0
    coef[0] = bar_re
    coef[1] = bar_im
    coef[2] = (lessened * lr + bar_im * li) / denom
    coef[3] = (bar_im * lr - lessened * li) / denom
    for load in loads[1:5]:
        load.wait()
    for load in block_loads:
        load.wait()
    gating[...] = jnp.zeros_like(gating)

    spread = iota((entries, span), 1) % entries == iota((entries, span), 0)
    mask = iota((128, span), 0) // channels == iota((128, span), 1) // entries
    pick = iota((span // entries, span), 0) == iota((span // entries, span), 1) // entries

    def expand(ref, j):
        part = ref[pl.ds(pl.multiple_of(j * 128, 128), 128), :].astype(BF16)
        tiled = jnp.dot(part, spread.astype(BF16), preferred_element_type=F32)
        return jnp.where(mask, tiled, 0.0).astype(BF16)

    def mix(j):
        block = held[pl.ds(j * unit, unit)].reshape(128, depth)
        inputs = lax.dot_general(normed[...], block, NT, preferred_element_type=F32).astype(BF16)
        drive_re = jnp.dot(inputs, expand(in_re, j), preferred_element_type=F32)
        drive_im = jnp.dot(inputs, expand(in_im, j), preferred_element_type=F32)
        per = span // entries
        rows = coef[:, pl.ds(pl.multiple_of(j * per, per), per), :].reshape(4 * per, entries)
        tiled = jnp.dot(rows, spread.astype(F32), precision=lax.Precision.HIGHEST, preferred_element_type=F32)
        line_of = [
            jnp.sum(jnp.where(pick, tiled[i * per : (i + 1) * per], 0.0), axis=0, keepdims=True) for i in range(4)
        ]
        old_re, old_im = state[0, :, column(j)], state[1, :, column(j)]
        new_re = line_of[0] * old_re - line_of[1] * old_im + (line_of[2] * drive_re - line_of[3] * drive_im)
        new_im = line_of[0] * old_im + line_of[1] * old_re + (line_of[2] * drive_im + line_of[3] * drive_re)
        state[0, :, column(j)] = new_re
        state[1, :, column(j)] = new_im
        read = lax.dot_general(new_re.astype(BF16), expand(out_re, j), NT, preferred_element_type=F32)
        read = read - lax.dot_general(new_im.astype(BF16), expand(out_im, j), NT, preferred_element_type=F32)
        lanes = pl.ds(pl.multiple_of(j * 128, 128), 128)
        act = jax.nn.gelu(read + skip_ref[:, lanes] * inputs.astype(F32))
        active[:, lanes] = act
        gating[...] += jnp.dot(act.astype(BF16), glu_w[lanes, :], preferred_element_type=F32)
        pltpu.make_async_copy(state.at[:, :, column(j)], new_any.at[:, :, column(j)], new_sems.at[j]).start()

    def place(item):
        kind, k = item
        if kind == 0:
            return order[k] * 2 + y
        return (line if k < 0 else order[k]) * 2 + 1 - y

    def take(item, p):
        kind, k = item
        s = line if k < 0 else order[k]
        spot = held.at[place(item), core, :, cols[p]]
        if kind == 0:
            remote(spot, spot, zs.at[s, p], zr.at[s, p], mate).wait_recv()
            start(remote(spot, spot, ys.at[s, p], yr.at[s, p], beside))
        else:
            remote(spot, spot, ys.at[s, p], yr.at[s, p], mate).wait_recv()
        if p == 0:
            start(remote(spot, spot, xs.at[place(item)], xr.at[place(item)], across))
        start(remote(spot, spot, ds.at[place(item), p], dr.at[place(item), p], mate))

    def take_x(item):
        spot = held.at[place(item), core, :, cols[2]]
        remote(spot, spot, xs.at[place(item)], xr.at[place(item)], mate).wait_recv()
        start(remote(spot, spot, ds.at[place(item), 2], dr.at[place(item), 2], mate))

    def settle(item):
        for p in range(3):
            spot = held.at[place(item), 1 - core, :, cols[p]]
            remote(spot, spot, ds.at[place(item), p], dr.at[place(item), p], mate).wait_recv()

    items = [(1, -1)]
    for k in range(lines):
        if k < lines - 1:
            items.append((0, k))
        if k > 0:
            items.append((1, k - 1))
    spot = held.at[chip, 1 - core]
    remote(spot, spot, own_s, own_r, mate).wait_recv()
    loads[5].wait()
    if unit == 1:
        mix(chip)
    for item in items:
        take(item, 0)
    ready = {-1: 1}
    for at_ in range(len(items) + 1):
        if at_ < len(items):
            take(items[at_], 1)
            if at_ == 0:
                continue
        take_x(items[at_ - 1])
        settle(items[at_ - 1])
        kind, k = items[at_ - 1]
        if unit == 1:
            mix(place(items[at_ - 1]))
        else:
            ready[k] = ready.get(k, 0) + 1
            if ready[k] == unit:
                mix(line if k < 0 else order[k])
    loads[6].wait()

    act = active[...]
    glu = (act * jax.nn.sigmoid(gating[...])).astype(BF16)
    resid = (hidden[...].astype(F32) + jnp.dot(glu, out_w[...], preferred_element_type=F32)).astype(BF16)
    resid_ref[...] = resid
    wide = resid.astype(F32)
    mean = jnp.mean(wide * wide, axis=-1, keepdims=True)
    second_normed = (wide * lax.rsqrt(mean + 1e-06) * ffn_gain_ref[...]).astype(BF16)
    rows_ref[:, :depth] = second_normed
    level = lax.dot_general(second_normed, w_group_ref[...], NT, preferred_element_type=F32)
    logits = lax.dot_general(second_normed, w_route_ref[...], NT, preferred_element_type=F32)
    count = second_normed.shape[0]
    lane = iota((count, 128), 1)
    same = (iota((count, count), 0) == iota((count, count), 1)).astype(BF16)
    ids = lax.dot_general(same, ids_ref[...].astype(F32).astype(BF16), NT, preferred_element_type=F32).astype(jnp.int32)
    first, second = ids[:, 0:1], ids[:, 1:2]
    group = first // per_group
    chosen = jnp.sum(jnp.where(iota(level.shape, 1) == group, level, 0.0), axis=1, keepdims=True)
    scale = 1.0 / jnp.sum(jnp.exp(level - chosen), axis=1, keepdims=True)
    r0 = jnp.sum(jnp.where(iota(logits.shape, 1) == first, logits, 0.0), axis=1, keepdims=True)
    r1 = jnp.sum(jnp.where(iota(logits.shape, 1) == second, logits, 0.0), axis=1, keepdims=True)
    share = jax.nn.sigmoid(r0 - r1)
    member = lane % per_group
    gate = jnp.where(member == first % per_group, scale * share, 0.0)
    gate = gate + jnp.where(member == second % per_group, scale * (1.0 - share), 0.0)
    high = gate.astype(BF16).astype(F32)
    packed = jnp.where(lane < per_group, high, jnp.where(lane < 2 * per_group, gate - high, 0.0))
    rows_ref[:, depth:] = packed.astype(BF16)
    hits = (lane == group).astype(BF16)
    earlier = (iota((count, count), 1) < iota((count, count), 0)).astype(BF16)
    before = jnp.dot(earlier, hits, preferred_element_type=F32)
    rank = jnp.sum(jnp.where(lane == group, before, 0.0), axis=1, keepdims=True).astype(jnp.int32)
    slots = place_ref.shape[1]
    slot = group * (slots // EXP_GROUPS) + rank
    place_ref[...] = (iota((count, slots), 1) == slot).astype(BF16)
    for j in range(blocks):
        columns = pl.ds(j * span, span)
        pltpu.make_async_copy(state.at[:, :, columns], new_any.at[:, :, columns], new_sems.at[j]).wait()
    for copy in sends:
        copy.wait_send()


def expert_kernel(
    groups, per_group, rows_ref, place_ref, resid_ref, gate_any, up_any, down_any, out_ref,
    outgoing, tokens, parts, parts_in, sums, sums_in, final, returned, w_gate, w_up, w_down,
    zs, zr, ys, yr, cs, cr, ps, pr, qs, qr, bs, br, w_sems,
):
    grp = lax.axis_index("grp")
    me = lax.axis_index("ep")
    pairs = per_group // 2
    g, p = me // per_group, me % per_group
    q, c = p // 2, p % 2
    depth = resid_ref.shape[1]
    cap = outgoing.shape[1]
    wide = outgoing.shape[2]

    def at(group, pair):
        return (grp, group * per_group + pair * 2 + c)

    mate = (grp, me + 1 - 2 * c)
    others = [(g + i) % groups for i in range(1, groups)]
    mates_q = [(q + j) % pairs for j in range(1, pairs)]
    loads = [
        pltpu.make_async_copy(gate_any.at[0], w_gate, w_sems.at[0]),
        pltpu.make_async_copy(up_any.at[0], w_up, w_sems.at[1]),
        pltpu.make_async_copy(down_any.at[0], w_down, w_sems.at[2]),
    ]
    for load in loads:
        load.start()
    sent = lax.dot_general(place_ref[...], rows_ref[...], TN, preferred_element_type=F32).astype(BF16)
    outgoing[...] = sent.reshape(groups, cap, wide)
    tokens[g, c, q] = outgoing[g]
    greet([at(o, q) for o in others] + [at(g, o) for o in mates_q] + [mate])
    sends = []

    def start(copy):
        copy.start()
        sends.append(copy)

    for target in others:
        start(remote(outgoing.at[target], tokens.at[g, c, q], zs.at[target], zr.at[g], at(target, q)))

    def source(i):
        return (g + groups - i) % groups

    def to_mate(s, pair):
        spot = tokens.at[s, c, pair]
        start(remote(spot, spot, cs.at[s, pair], cr.at[s, pair], mate))

    def stage_a(i):
        s = source(i)
        spot = tokens.at[s, c, q]
        if i > 0:
            remote(spot, spot, zs.at[s], zr.at[s], mate).wait_recv()
        for o in mates_q:
            start(remote(spot, spot, ys.at[s, o], yr.at[s, q], at(g, o)))
        to_mate(s, q)

    def stage_b(i):
        s = source(i)
        for o in mates_q:
            spot = tokens.at[s, c, o]
            remote(spot, spot, ys.at[s, o], yr.at[s, o], mate).wait_recv()
            to_mate(s, o)

    def stage_c(i):
        s = source(i)
        for o in range(pairs):
            spot = tokens.at[s, 1 - c, o]
            remote(spot, spot, cs.at[s, o], cr.at[s, o], mate).wait_recv()
        if i == 0:
            for load in loads:
                load.wait()
        total = per_group * cap
        x = tokens[s].reshape(total, wide)
        rows = x[:, :depth]
        gate = jnp.dot(rows, w_gate[...], preferred_element_type=F32)
        upper = jnp.dot(rows, w_up[...], preferred_element_type=F32)
        inner = (jax.nn.silu(gate) * upper).astype(BF16)
        result = jnp.dot(inner, w_down[...], preferred_element_type=F32).astype(BF16)
        lane = lax.broadcasted_iota(jnp.int32, (total, wide - depth), 1)
        mine = (lane == p) | (lane == p + per_group)
        weight = jnp.sum(jnp.where(mine, x[:, depth:].astype(F32), 0.0), axis=1, keepdims=True)
        parts[s] = (result.astype(F32) * weight).astype(BF16).reshape(2, pairs, cap, depth)
        start(remote(parts.at[s, 1 - c], parts_in.at[s], ps.at[s], pr.at[s], mate))

    def stage_d(i):
        s = source(i)
        spot = parts_in.at[s]
        remote(spot, spot, ps.at[s], pr.at[s], mate).wait_recv()
        sums[s] = (parts[s, c].astype(F32) + parts_in[s].astype(F32)).astype(BF16)
        for o in mates_q:
            start(remote(sums.at[s, o], sums_in.at[s, q], qs.at[s, o], qr.at[s, q], at(g, o)))

    def stage_e(i):
        s = source(i)
        total = sums[s, q].astype(F32)
        for o in mates_q:
            spot = sums_in.at[s, o]
            remote(spot, spot, qs.at[s, o], qr.at[s, o], mate).wait_recv()
            total = total + sums_in[s, o].astype(F32)
        if i == 0:
            returned[g] = total.astype(BF16)
        else:
            final[s] = total.astype(BF16)
            start(remote(final.at[s], returned.at[g], bs.at[s], br.at[g], at(s, q)))

    stage_a(0)
    for t in range(groups):
        stage_b(t)
        if t + 1 < groups:
            stage_a(t + 1)
        stage_c(t)
        stage_d(t)
        if t > 0:
            stage_e(t - 1)
    stage_e(groups - 1)
    for o in others:
        spot = returned.at[o]
        remote(spot, spot, bs.at[o], br.at[o], mate).wait_recv()
    back = returned[...].reshape(groups * cap, depth)
    moe = jnp.dot(place_ref[...], back, preferred_element_type=F32)
    out_ref[...] = (resid_ref[...].astype(F32) + moe).astype(BF16)
    for copy in sends:
        copy.wait_send()


def on_device(
    hidden, state, norm_gain, w_in, lam_re, lam_im, log_step, in_re, in_im, out_re, out_im, skip, w_glu, w_out,
    ffn_gain, w_group, w_route, w_gate, w_up, w_down, route_ids,
):
    rows, depth = hidden.shape
    devices = lax.axis_size("ep")
    chips = devices // 2
    shard = w_in.shape[1]
    dma = pltpu.SemaphoreType.DMA
    groups, entries = lam_re.shape
    width = in_re.shape[2]
    channels = groups * width
    lines = chips // 2
    blocks = channels // 128
    experts = w_route.shape[1]
    per_group = experts // EXP_GROUPS
    cap = 2 * rows // EXP_GROUPS
    new_state, resid, packed, place = pl.pallas_call(
        functools.partial(front_kernel, chips, per_group),
        out_shape=[
            jax.ShapeDtypeStruct(state.shape, F32),
            jax.ShapeDtypeStruct((rows, depth), BF16),
            jax.ShapeDtypeStruct((rows, depth + 128), BF16),
            jax.ShapeDtypeStruct((rows, EXP_GROUPS * cap), BF16),
        ],
        in_specs=[ANY, VMEM, ANY, ANY] + [VMEM] * 3 + [ANY] * 4 + [VMEM] * 2 + [ANY] * 2 + [VMEM] * 3,
        out_specs=[ANY] + [VMEM] * 3,
        scratch_shapes=[
            pltpu.VMEM((chips, 2, shard, depth), BF16),
            pltpu.VMEM((rows, depth), BF16),
            pltpu.VMEM(state.shape, F32),
        ] + [pltpu.VMEM((channels, entries), F32)] * 4 + [
            pltpu.VMEM(w_glu.shape, BF16),
            pltpu.VMEM(w_out.shape, BF16),
            pltpu.VMEM((rows, depth), BF16),
            pltpu.VMEM((4, groups, entries), F32),
            pltpu.VMEM((rows, channels), F32),
            pltpu.VMEM((rows, channels), F32),
        ] + [dma((lines, 2))] * 4 + [dma((chips,))] * 2 + [dma((chips, 3))] * 2
        + [dma, dma, dma((8,)), dma((blocks,)), dma((blocks,))],
        compiler_params=pltpu.CompilerParams(collective_id=0, has_side_effects=True, vmem_limit_bytes=FRONT_LIMIT),
        name="front",
    )(
        hidden, norm_gain[None, :], w_in.T, state, lam_re, lam_im, log_step[None, :],
        in_re.transpose(0, 2, 1).reshape(channels, entries), in_im.transpose(0, 2, 1).reshape(channels, entries),
        out_re.reshape(channels, entries), out_im.reshape(channels, entries), skip[None, :], ffn_gain[None, :],
        w_glu, w_out, w_group.T, w_route.T, route_ids.T,
    )

    pairs = per_group // 2
    G = EXP_GROUPS
    hidden_out = pl.pallas_call(
        functools.partial(expert_kernel, G, per_group),
        out_shape=jax.ShapeDtypeStruct((rows, depth), BF16),
        in_specs=[VMEM] * 3 + [ANY] * 3,
        out_specs=VMEM,
        scratch_shapes=[
            pltpu.VMEM((G, cap, depth + 128), BF16),
            pltpu.VMEM((G, 2, pairs, cap, depth + 128), BF16),
            pltpu.VMEM((G, 2, pairs, cap, depth), BF16),
            pltpu.VMEM((G, pairs, cap, depth), BF16),
            pltpu.VMEM((G, pairs, cap, depth), BF16),
            pltpu.VMEM((G, pairs, cap, depth), BF16),
            pltpu.VMEM((G, cap, depth), BF16),
            pltpu.VMEM((G, cap, depth), BF16),
            pltpu.VMEM(w_gate.shape[1:], BF16),
            pltpu.VMEM(w_up.shape[1:], BF16),
            pltpu.VMEM(w_down.shape[1:], BF16),
            dma((G,)), dma((G,)), dma((G, pairs)), dma((G, pairs)), dma((G, pairs)), dma((G, pairs)),
            dma((G,)), dma((G,)), dma((G, pairs)), dma((G, pairs)), dma((G,)), dma((G,)), dma((3,)),
        ],
        compiler_params=pltpu.CompilerParams(collective_id=1, has_side_effects=True, vmem_limit_bytes=LIMIT),
        name="experts",
    )(packed, place, resid, w_gate, w_up, w_down)
    return (hidden_out, new_state)


def solution(mesh):
    return jax.shard_map(
        on_device,
        mesh=mesh,
        in_specs=(
            P(("grp", "ep"), None),
            P(None, ("grp", "ep"), None),
            P(),
            P(None, "ep"),
            P(),
            P(),
            P(),
            P(),
            P(),
            P(),
            P(),
            P(),
            P(),
            P(),
            P(),
            P(),
            P(),
            P("ep", None, None),
            P("ep", None, None),
            P("ep", None, None),
            P(("grp", "ep"), None),
        ),
        out_specs=(P(("grp", "ep"), None), P(None, ("grp", "ep"), None)),
        check_vma=False,
    )
```

```python
import functools

import jax
import jax.numpy as jnp
from jax import lax
from jax.experimental import pallas as pl
from jax.experimental.pallas import tpu as pltpu
from jax.sharding import PartitionSpec as P

EXP_GROUPS = 4
TOPK = 2
MESH = pl.DeviceIdType.MESH
VMEM = pl.BlockSpec(memory_space=pltpu.VMEM)
ANY = pl.BlockSpec(memory_space=pl.ANY)
F32 = jnp.float32
BF16 = jnp.bfloat16
NT = (((1,), (1,)), ((), ()))
TN = (((0,), (0,)), ((), ()))
LIMIT = 57 * 1024 * 1024
FINISH_LIMIT = 16 * 1024 * 1024


def remote(src, dst, send_sem, recv_sem, device):
    return pltpu.make_async_remote_copy(
        src_ref=src, dst_ref=dst, send_sem=send_sem, recv_sem=recv_sem, device_id=device, device_id_type=MESH
    )


def greet(peers):
    barrier = pltpu.get_barrier_semaphore()
    for peer in peers:
        pl.semaphore_signal(barrier, inc=1, device_id=peer, device_id_type=MESH)
    pl.semaphore_wait(barrier, len(peers))


def nearest(spot, count, k):
    after = count - 1 - spot
    longer = (after - spot + count - 1) // count
    short = spot * longer + after * (1 - longer)
    past = (k + 2 * count - 2 * short) // (2 * count)
    paired = (k // 2 + 1) * (1 - 2 * (k % 2))
    single = (k - short + 1) * (2 * longer - 1)
    return spot + paired * (1 - past) + single * past


def front(
    chips, per_group, sends, hidden_any, gain_ref, w_any, state_any, lam_re_ref, lam_im_ref, step_ref, in_re_any, in_im_any,
    out_re_any, out_im_any, skip_ref, ffn_gain_ref, w_glu_any, w_out_any, w_group_ref, w_route_ref, ids_ref,
    state, resid_ref, place_ref, rows_ref,
    held, hidden, in_re, in_im, out_re, out_im, glu_w, out_w, normed, coef, active, gating,
    zs, zr, ys, yr, xs, xr, ds, dr, own_s, own_r, load_sems, state_sems, meet, expert_loads,
):
    grp = lax.axis_index("grp")
    me = lax.axis_index("ep")
    chip, core = me // 2, me % 2
    lines = chips // 2
    line, y = chip // 2, chip % 2
    side = grp % 2
    shard, depth = w_any.shape
    entries = lam_re_ref.shape[1]
    unit = 128 // (2 * shard)
    blocks = chips // unit
    span = state.shape[2] // blocks
    channels = 128 // (span // entries)

    def at(row, column):
        return (grp, (row * 2 + column) * 2 + core)

    mate = (grp, me + 1 - 2 * core)
    across = (grp + 1 - 2 * side, me)
    beside = at(line, 1 - y)
    order = [nearest(line, lines, k) for k in range(lines - 1)]
    third = depth // 3 // 128 * 128
    middle = depth - 2 * third
    cols = [
        pl.ds(pl.multiple_of(side * (depth - third), 128), third),
        pl.ds(third, middle),
        pl.ds(pl.multiple_of((1 - side) * (depth - third), 128), third),
    ]

    def start(copy):
        copy.start()
        sends.append(copy)

    def column(j):
        return pl.ds(pl.multiple_of(j * span, 128), span)

    own = pltpu.make_async_copy(w_any, held.at[chip, core], load_sems.at[0])
    own.start()
    loads = [
        pltpu.make_async_copy(src, dst, load_sems.at[1 + i])
        for i, (src, dst) in enumerate([
            (hidden_any, hidden), (in_re_any, in_re), (in_im_any, in_im), (out_re_any, out_re), (out_im_any, out_im),
            (w_glu_any, glu_w), (w_out_any, out_w),
        ])
    ]
    for load in loads[:1]:
        load.start()
    meet([at(o, y) for o in order] + [beside, mate, across])
    own.wait()
    for p in range(2):
        spot = held.at[chip, core, :, cols[p]]
        start(remote(spot, spot, ys.at[line, p], yr.at[line, p], beside))
        for o in order:
            start(remote(spot, spot, zs.at[o, p], zr.at[line, p], at(o, y)))
    spot = held.at[chip, core]
    start(remote(spot, spot, own_s, own_r, mate))
    for load in loads[1:]:
        load.start()
    block_loads = [
        pltpu.make_async_copy(state_any.at[:, :, pl.ds(j * span, span)], state.at[:, :, pl.ds(j * span, span)], state_sems.at[j])
        for j in range(blocks)
    ]
    for load in block_loads + expert_loads:
        load.start()

    def iota(shape, axis):
        return lax.broadcasted_iota(jnp.int32, shape, axis)

    loads[0].wait()
    wide = hidden[...].astype(F32)
    mean = jnp.mean(wide * wide, axis=-1, keepdims=True)
    normed[...] = (wide * lax.rsqrt(mean + 1e-06) * gain_ref[...]).astype(BF16)

    groups = lam_re_ref.shape[0]
    lr, li = lam_re_ref[...], lam_im_ref[...]
    diagonal = iota((groups, groups), 0) == iota((groups, groups), 1)
    step = jnp.exp(jnp.sum(jnp.where(diagonal, step_ref[...], 0.0), axis=1, keepdims=True))
    magnitude = jnp.exp(lr * step)
    bar_re = magnitude * jnp.cos(li * step)
    bar_im = magnitude * jnp.sin(li * step)
    denom = lr * lr + li * li
    lessened = bar_re - 1.0
    coef[0] = bar_re
    coef[1] = bar_im
    coef[2] = (lessened * lr + bar_im * li) / denom
    coef[3] = (bar_im * lr - lessened * li) / denom
    for load in loads[1:5]:
        load.wait()
    for load in block_loads:
        load.wait()
    gating[...] = jnp.zeros_like(gating)

    spread = iota((entries, span), 1) % entries == iota((entries, span), 0)
    mask = iota((128, span), 0) // channels == iota((128, span), 1) // entries
    pick = iota((span // entries, span), 0) == iota((span // entries, span), 1) // entries

    def expand(ref, j):
        part = ref[pl.ds(pl.multiple_of(j * 128, 128), 128), :].astype(BF16)
        tiled = jnp.dot(part, spread.astype(BF16), preferred_element_type=F32)
        return jnp.where(mask, tiled, 0.0).astype(BF16)

    def mix(j):
        block = held[pl.ds(j * unit, unit)].reshape(128, depth)
        inputs = lax.dot_general(normed[...], block, NT, preferred_element_type=F32).astype(BF16)
        drive_re = jnp.dot(inputs, expand(in_re, j), preferred_element_type=F32)
        drive_im = jnp.dot(inputs, expand(in_im, j), preferred_element_type=F32)
        per = span // entries
        rows = coef[:, pl.ds(pl.multiple_of(j * per, per), per), :].reshape(4 * per, entries)
        tiled = jnp.dot(rows, spread.astype(F32), precision=lax.Precision.HIGHEST, preferred_element_type=F32)
        line_of = [
            jnp.sum(jnp.where(pick, tiled[i * per : (i + 1) * per], 0.0), axis=0, keepdims=True) for i in range(4)
        ]
        old_re, old_im = state[0, :, column(j)], state[1, :, column(j)]
        new_re = line_of[0] * old_re - line_of[1] * old_im + (line_of[2] * drive_re - line_of[3] * drive_im)
        new_im = line_of[0] * old_im + line_of[1] * old_re + (line_of[2] * drive_im + line_of[3] * drive_re)
        state[0, :, column(j)] = new_re
        state[1, :, column(j)] = new_im
        read = lax.dot_general(new_re.astype(BF16), expand(out_re, j), NT, preferred_element_type=F32)
        read = read - lax.dot_general(new_im.astype(BF16), expand(out_im, j), NT, preferred_element_type=F32)
        lanes = pl.ds(pl.multiple_of(j * 128, 128), 128)
        act = jax.nn.gelu(read + skip_ref[:, lanes] * inputs.astype(F32))
        active[:, lanes] = act
        gating[...] += jnp.dot(act.astype(BF16), glu_w[lanes, :], preferred_element_type=F32)

    def place(item):
        kind, k = item
        if kind == 0:
            return order[k] * 2 + y
        return (line if k < 0 else order[k]) * 2 + 1 - y

    def take(item, p):
        kind, k = item
        s = line if k < 0 else order[k]
        spot = held.at[place(item), core, :, cols[p]]
        if kind == 0:
            remote(spot, spot, zs.at[s, p], zr.at[s, p], mate).wait_recv()
            start(remote(spot, spot, ys.at[s, p], yr.at[s, p], beside))
        else:
            remote(spot, spot, ys.at[s, p], yr.at[s, p], mate).wait_recv()
        if p == 0:
            start(remote(spot, spot, xs.at[place(item)], xr.at[place(item)], across))
        start(remote(spot, spot, ds.at[place(item), p], dr.at[place(item), p], mate))

    def take_x(item):
        spot = held.at[place(item), core, :, cols[2]]
        remote(spot, spot, xs.at[place(item)], xr.at[place(item)], mate).wait_recv()
        start(remote(spot, spot, ds.at[place(item), 2], dr.at[place(item), 2], mate))

    def settle(item):
        for p in range(3):
            spot = held.at[place(item), 1 - core, :, cols[p]]
            remote(spot, spot, ds.at[place(item), p], dr.at[place(item), p], mate).wait_recv()

    items = [(1, -1)]
    for k in range(lines):
        if k < lines - 1:
            items.append((0, k))
        if k > 0:
            items.append((1, k - 1))
    spot = held.at[chip, 1 - core]
    remote(spot, spot, own_s, own_r, mate).wait_recv()
    loads[5].wait()
    if unit == 1:
        mix(chip)
    for item in items:
        take(item, 0)
    ready = {-1: 1}
    for at_ in range(len(items) + 1):
        if at_ < len(items):
            take(items[at_], 1)
            if at_ == 0:
                continue
        take_x(items[at_ - 1])
        settle(items[at_ - 1])
        kind, k = items[at_ - 1]
        if unit == 1:
            mix(place(items[at_ - 1]))
        else:
            ready[k] = ready.get(k, 0) + 1
            if ready[k] == unit:
                mix(line if k < 0 else order[k])
    loads[6].wait()

    act = active[...]
    glu = (act * jax.nn.sigmoid(gating[...])).astype(BF16)
    resid = (hidden[...].astype(F32) + jnp.dot(glu, out_w[...], preferred_element_type=F32)).astype(BF16)
    resid_ref[...] = resid
    wide = resid.astype(F32)
    mean = jnp.mean(wide * wide, axis=-1, keepdims=True)
    second_normed = (wide * lax.rsqrt(mean + 1e-06) * ffn_gain_ref[...]).astype(BF16)
    rows_ref[:, :depth] = second_normed
    level = lax.dot_general(second_normed, w_group_ref[...], NT, preferred_element_type=F32)
    logits = lax.dot_general(second_normed, w_route_ref[...], NT, preferred_element_type=F32)
    count = second_normed.shape[0]
    lane = iota((count, 128), 1)
    same = (iota((count, count), 0) == iota((count, count), 1)).astype(BF16)
    ids = lax.dot_general(same, ids_ref[...].astype(F32).astype(BF16), NT, preferred_element_type=F32).astype(jnp.int32)
    first, second = ids[:, 0:1], ids[:, 1:2]
    group = first // per_group
    chosen = jnp.sum(jnp.where(iota(level.shape, 1) == group, level, 0.0), axis=1, keepdims=True)
    scale = 1.0 / jnp.sum(jnp.exp(level - chosen), axis=1, keepdims=True)
    r0 = jnp.sum(jnp.where(iota(logits.shape, 1) == first, logits, 0.0), axis=1, keepdims=True)
    r1 = jnp.sum(jnp.where(iota(logits.shape, 1) == second, logits, 0.0), axis=1, keepdims=True)
    share = jax.nn.sigmoid(r0 - r1)
    member = lane % per_group
    gate = jnp.where(member == first % per_group, scale * share, 0.0)
    gate = gate + jnp.where(member == second % per_group, scale * (1.0 - share), 0.0)
    high = gate.astype(BF16).astype(F32)
    packed = jnp.where(lane < per_group, high, jnp.where(lane < 2 * per_group, gate - high, 0.0))
    rows_ref[:, depth:] = packed.astype(BF16)
    hits = (lane == group).astype(BF16)
    earlier = (iota((count, count), 1) < iota((count, count), 0)).astype(BF16)
    before = jnp.dot(earlier, hits, preferred_element_type=F32)
    rank = jnp.sum(jnp.where(lane == group, before, 0.0), axis=1, keepdims=True).astype(jnp.int32)
    slots = place_ref.shape[1]
    slot = group * (slots // EXP_GROUPS) + rank
    place_ref[...] = (iota((count, slots), 1) == slot).astype(BF16)


def experts(
    groups, per_group, subs, sends, rows_ref, place_ref, returned,
    outgoing, tokens, parts, parts_in, sums, sums_in, final, w_gate, w_up, w_down,
    zs, zr, ys, yr, cs, cr, ps, pr, qs, qr, bs, br, loads,
):
    grp = lax.axis_index("grp")
    me = lax.axis_index("ep")
    pairs = per_group // 2
    g, p = me // per_group, me % per_group
    q, c = p // 2, p % 2
    depth = returned.shape[2]
    cap = outgoing.shape[1]
    wide = outgoing.shape[2]
    part = cap // subs
    spans = [pl.ds(i * part, part) for i in range(subs)]

    def at(group, pair):
        return (grp, group * per_group + pair * 2 + c)

    mate = (grp, me + 1 - 2 * c)
    half = groups // 2
    low = g // half * half
    crossing = [(low + half) % groups + (g + i) % half for i in range(half)]
    inside = [low + (g + i) % half for i in range(1, half)]
    sources = [g] + inside + crossing
    others = sources[1:]
    mates_q = [(q + j) % pairs for j in range(1, pairs)]
    sent = lax.dot_general(place_ref[...], rows_ref[...], TN, preferred_element_type=F32).astype(BF16)
    outgoing[...] = sent.reshape(groups, cap, wide)
    tokens[g, c, q] = outgoing[g]

    def start(copy):
        copy.start()
        sends.append(copy)

    for u in range(subs):
        for target in others:
            start(remote(
                outgoing.at[target, spans[u]], tokens.at[g, c, q, spans[u]], zs.at[target, u], zr.at[g, u], at(target, q)
            ))

    def spread(k, u):
        s = sources[k]
        spot = tokens.at[s, c, q, spans[u]]
        if k > 0:
            remote(spot, spot, zs.at[s, u], zr.at[s, u], mate).wait_recv()
        for o in mates_q:
            start(remote(spot, spot, ys.at[s, o, u], yr.at[s, q, u], at(g, o)))
        start(remote(spot, spot, cs.at[s, q, u], cr.at[s, q, u], mate))

    def relay(k, u):
        s = sources[k]
        for o in mates_q:
            spot = tokens.at[s, c, o, spans[u]]
            remote(spot, spot, ys.at[s, o, u], yr.at[s, o, u], mate).wait_recv()
            start(remote(spot, spot, cs.at[s, o, u], cr.at[s, o, u], mate))

    def compute(k, u):
        s = sources[k]
        for o in range(pairs):
            spot = tokens.at[s, 1 - c, o, spans[u]]
            remote(spot, spot, cs.at[s, o, u], cr.at[s, o, u], mate).wait_recv()
        if k == 0 and u == 0:
            for load in loads:
                load.wait()
        total = per_group * part
        x = tokens[s, :, :, spans[u]].reshape(total, wide)
        rows = x[:, :depth]
        gate = jnp.dot(rows, w_gate[...], preferred_element_type=F32)
        upper = jnp.dot(rows, w_up[...], preferred_element_type=F32)
        inner = (jax.nn.silu(gate) * upper).astype(BF16)
        result = jnp.dot(inner, w_down[...], preferred_element_type=F32).astype(BF16)
        lane = lax.broadcasted_iota(jnp.int32, (total, wide - depth), 1)
        mine = (lane == p) | (lane == p + per_group)
        weight = jnp.sum(jnp.where(mine, x[:, depth:].astype(F32), 0.0), axis=1, keepdims=True)
        parts[s, u] = (result.astype(F32) * weight).astype(BF16).reshape(2, pairs, part, depth)
        start(remote(parts.at[s, u, 1 - c], parts_in.at[s, u], ps.at[s, u], pr.at[s, u], mate))

    def reduce_mate(k, u):
        s = sources[k]
        spot = parts_in.at[s, u]
        remote(spot, spot, ps.at[s, u], pr.at[s, u], mate).wait_recv()
        sums[s, u] = (parts[s, u, c].astype(F32) + parts_in[s, u].astype(F32)).astype(BF16)
        for o in mates_q:
            start(remote(sums.at[s, u, o], sums_in.at[s, u, q], qs.at[s, o, u], qr.at[s, q, u], at(g, o)))

    def reduce_pairs(k, u):
        s = sources[k]
        total = sums[s, u, q].astype(F32)
        for o in mates_q:
            spot = sums_in.at[s, u, o]
            remote(spot, spot, qs.at[s, o, u], qr.at[s, o, u], mate).wait_recv()
            total = total + sums_in[s, u, o].astype(F32)
        if k == 0:
            returned[g, spans[u]] = total.astype(BF16)
        else:
            final[s, spans[u]] = total.astype(BF16)
            start(remote(
                final.at[s, spans[u]], returned.at[g, spans[u]], bs.at[s, u], br.at[g, u], at(s, q)
            ))

    every = range(subs)
    own, near, far = [0], list(range(1, half)), list(range(half, groups))
    early, late = every[:1], every[1:]

    def run(stage, kinds, units):
        for u in units:
            for k in kinds:
                stage(k, u)

    run(spread, own, every)
    run(spread, near, early)
    run(relay, own, every)
    run(spread, far[:1], early)
    run(compute, own, early)
    run(spread, far[1:], early)
    run(compute, own, late)
    run(relay, near, early)
    run(relay, far[:1], early)
    run(compute, far[:1], early)
    run(spread, near, late)
    run(relay, far[1:], early)
    run(compute, far[1:], early)
    run(reduce_mate, far[:1], early)
    run(spread, far[:1], late)
    run(reduce_mate, far[1:], early)
    run(spread, far[1:], late)
    run(compute, near, early)
    run(reduce_pairs, far, early)
    run(reduce_mate, near, early)
    run(relay, near, late)
    run(relay, far[:1], late)
    run(compute, far[:1], late)
    run(relay, far[1:], late)
    run(compute, far[1:], late)
    run(reduce_mate, far, late)
    run(compute, near, late)
    run(reduce_pairs, far, late)
    run(reduce_mate, near, late)
    run(reduce_mate, own, every)
    run(reduce_pairs, near, every)
    run(reduce_pairs, own, every)
    for o in others:
        for u in every:
            spot = returned.at[o, spans[u]]
            remote(spot, spot, bs.at[o, u], br.at[o, u], mate).wait_recv()


def layer_kernel(
    chips, groups, per_group, subs, *refs,
):
    inputs, outputs, scratch = refs[:21], refs[21:25], refs[25:]
    weights = inputs[18:]
    state, resid_ref, place_ref, returned = outputs
    rows_ref, *rest = scratch
    front_scratch, rest = rest[:12], rest[12:]
    front_sems, rest = rest[:12], rest[12:]
    expert_scratch, expert_sems = rest[:10], rest[10:]
    loads = [
        pltpu.make_async_copy(src.at[0], dst, expert_sems[-1].at[i])
        for i, (src, dst) in enumerate(zip(weights, expert_scratch[7:]))
    ]
    sends = []

    def meet(peers):
        grp = lax.axis_index("grp")
        me = lax.axis_index("ep")
        g, p = me // per_group, me % per_group
        ahead = [(grp, (g + i) % groups * per_group + p) for i in range(1, groups)]
        near = [(grp, g * per_group + (p + 2 * i) % per_group) for i in range(1, per_group // 2)]
        greet(peers + ahead + near)

    front(
        chips, per_group, sends, *inputs[:18], state, resid_ref, place_ref, rows_ref, *front_scratch, *front_sems,
        meet, loads,
    )
    experts(
        groups, per_group, subs, sends, rows_ref, place_ref, returned, *expert_scratch, *expert_sems[:-1], loads,
    )
    for copy in sends:
        copy.wait_send()


def finish_kernel(state_ref, resid_ref, place_ref, returned_ref, new_any, out_ref, sems):
    copies = [
        pltpu.make_async_copy(
            state_ref.at[i, pl.ds(j * 64, 64)], new_any.at[i, pl.ds(j * 64, 64)], sems.at[i, j]
        )
        for i in range(2) for j in range(state_ref.shape[1] // 64)
    ]
    for copy in copies:
        copy.start()
    back = returned_ref[...].reshape(-1, returned_ref.shape[2])
    moe = jnp.dot(place_ref[...], back, preferred_element_type=F32)
    out_ref[...] = (resid_ref[...].astype(F32) + moe).astype(BF16)
    for copy in copies:
        copy.wait()


def on_device(
    hidden, state, norm_gain, w_in, lam_re, lam_im, log_step, in_re, in_im, out_re, out_im, skip, w_glu, w_out,
    ffn_gain, w_group, w_route, w_gate, w_up, w_down, route_ids,
):
    rows, depth = hidden.shape
    devices = lax.axis_size("ep")
    chips = devices // 2
    shard = w_in.shape[1]
    dma = pltpu.SemaphoreType.DMA
    groups, entries = lam_re.shape
    width = in_re.shape[2]
    channels = groups * width
    lines = chips // 2
    blocks = channels // 128
    experts = w_route.shape[1]
    per_group = experts // EXP_GROUPS
    cap = 2 * rows // EXP_GROUPS
    pairs = per_group // 2
    G = EXP_GROUPS
    subs = cap // 32
    part = cap // subs
    vm = pltpu.VMEM
    kept = [
        vm(state.shape, F32), vm((rows, depth), BF16), vm((rows, G * cap), BF16), vm((G, cap, depth), BF16),
    ]
    results = pl.pallas_call(
        functools.partial(layer_kernel, chips, G, per_group, subs),
        out_shape=kept,
        in_specs=[ANY, VMEM, ANY, ANY] + [VMEM] * 3 + [ANY] * 4 + [VMEM] * 2 + [ANY] * 2 + [VMEM] * 3 + [ANY] * 3,
        out_specs=[VMEM] * 4,
        scratch_shapes=[
            vm((rows, depth + 128), BF16),
            vm((chips, 2, shard, depth), BF16),
            vm((rows, depth), BF16),
        ] + [vm((channels, entries), F32)] * 4 + [
            vm(w_glu.shape, BF16),
            vm(w_out.shape, BF16),
            vm((rows, depth), BF16),
            vm((4, groups, entries), F32),
            vm((rows, channels), F32),
            vm((rows, channels), F32),
        ] + [dma((lines, 2))] * 4 + [dma((chips,))] * 2 + [dma((chips, 3))] * 2
        + [dma, dma, dma((8,)), dma((blocks,))] + [
            vm((G, cap, depth + 128), BF16),
            vm((G, 2, pairs, cap, depth + 128), BF16),
            vm((G, subs, 2, pairs, part, depth), BF16),
            vm((G, subs, pairs, part, depth), BF16),
            vm((G, subs, pairs, part, depth), BF16),
            vm((G, subs, pairs, part, depth), BF16),
            vm((G, cap, depth), BF16),
            vm(w_gate.shape[1:], BF16),
            vm(w_up.shape[1:], BF16),
            vm(w_down.shape[1:], BF16),
        ] + [dma((G, subs))] * 2 + [dma((G, pairs, subs))] * 4 + [dma((G, subs))] * 2 + [dma((G, pairs, subs))] * 2
        + [dma((G, subs))] * 2 + [dma((3,))],
        compiler_params=pltpu.CompilerParams(collective_id=0, has_side_effects=True, vmem_limit_bytes=LIMIT),
        name="layer",
    )(
        hidden, norm_gain[None, :], w_in.T, state, lam_re, lam_im, log_step[None, :],
        in_re.transpose(0, 2, 1).reshape(channels, entries), in_im.transpose(0, 2, 1).reshape(channels, entries),
        out_re.reshape(channels, entries), out_im.reshape(channels, entries), skip[None, :], ffn_gain[None, :],
        w_glu, w_out, w_group.T, w_route.T, route_ids.T, w_gate, w_up, w_down,
    )
    new_state, hidden_out = pl.pallas_call(
        finish_kernel,
        out_shape=[jax.ShapeDtypeStruct(state.shape, F32), jax.ShapeDtypeStruct((rows, depth), BF16)],
        in_specs=[VMEM] * 4,
        out_specs=[ANY, VMEM],
        scratch_shapes=[dma((2, rows // 64))],
        compiler_params=pltpu.CompilerParams(vmem_limit_bytes=FINISH_LIMIT),
        name="finish",
    )(*results)
    return (hidden_out, new_state)


def solution(mesh):
    return jax.shard_map(
        on_device,
        mesh=mesh,
        in_specs=(
            P(("grp", "ep"), None),
            P(None, ("grp", "ep"), None),
            P(),
            P(None, "ep"),
            P(),
            P(),
            P(),
            P(),
            P(),
            P(),
            P(),
            P(),
            P(),
            P(),
            P(),
            P(),
            P(),
            P("ep", None, None),
            P("ep", None, None),
            P("ep", None, None),
            P(("grp", "ep"), None),
        ),
        out_specs=(P(("grp", "ep"), None), P(None, ("grp", "ep"), None)),
        check_vma=False,
    )
```

```python
import functools

import jax
import jax.numpy as jnp
from jax import lax
from jax.experimental import pallas as pl
from jax.experimental.pallas import tpu as pltpu
from jax.sharding import PartitionSpec as P

EXP_GROUPS = 4
TOPK = 2
MESH = pl.DeviceIdType.MESH
VMEM = pl.BlockSpec(memory_space=pltpu.VMEM)
ANY = pl.BlockSpec(memory_space=pl.ANY)
F32 = jnp.float32
BF16 = jnp.bfloat16
NT = (((1,), (1,)), ((), ()))
TN = (((0,), (0,)), ((), ()))
GATHER_ORDER = (
    "o0 a0 o1 a1", "b0 c0 b1 a2", "o2 a4 o5 A0", "o4 o3 A1 B0", "a3 a5 b2 om", "b4 c1 B1 b5",
    "c4 b3 am c3", "A3 A4 A2 C0", "A5 bm c2 C1", "B4 c5 B2 B3", "B5 Am C4 Bm", "C3 C5 C2 cm",
    "Cm",
)
SEND_ORDER = (
    "20 10 30 21", "11 31 13 12", "22 23 32 33",
)
EXPERT_ORDER = (
    "F00 F02 F01 G00", "F03 G02 G01 F20", "G03 F10 F30 C00", "F21 C01 G20 F11", "F31 F13 G30 G21", "G10 F12 C20 F22",
    "G11 M20 G31 F23", "C10 M21 C30 E20", "G13 F32 G22 G12", "G23 M30 F33 E21", "C21 M31 M10 G32", "E30 C11 M22 G33",
    "M11 M23 E31 C31", "E22 E10 M12 M32", "M33 E23 M00 M13", "M02 E11 E32 E12", "M03 M01 E33 E13", "E03 E02 E00 E01",
)
LIMIT = 57 * 1024 * 1024
FINISH_LIMIT = 16 * 1024 * 1024


def remote(src, dst, send_sem, recv_sem, device):
    return pltpu.make_async_remote_copy(
        src_ref=src, dst_ref=dst, send_sem=send_sem, recv_sem=recv_sem, device_id=device, device_id_type=MESH
    )


def greet(peers):
    barrier = pltpu.get_barrier_semaphore()
    for peer in peers:
        pl.semaphore_signal(barrier, inc=1, device_id=peer, device_id_type=MESH)
    pl.semaphore_wait(barrier, len(peers))


def words(table):
    return [word for text in table for word in text.split()]


def front(
    chips, per_group, sends, hidden_any, gain_ref, w_any, state_any, lam_re_ref, lam_im_ref, step_ref, in_re_any, in_im_any,
    out_re_any, out_im_any, skip_ref, ffn_gain_ref, w_glu_any, w_out_any, w_group_ref, w_route_ref, ids_ref,
    state, resid_ref, place_ref, rows_ref,
    held, hidden, in_re, in_im, out_re, out_im, glu_w, out_w, normed, coef, active, gating,
    zs, zr, ys, yr, xs, xr, ds, dr, fs, own_s, own_r, load_sems, state_sems, meet, expert_loads,
):
    grp = lax.axis_index("grp")
    me = lax.axis_index("ep")
    chip, core = me // 2, me % 2
    lines = chips // 2
    line, y = chip // 2, chip % 2
    side = grp % 2
    shard, depth = w_any.shape
    entries = lam_re_ref.shape[1]
    unit = 128 // (2 * shard)
    blocks = chips // unit
    span = state.shape[2] // blocks
    channels = 128 // (span // entries)

    def at(row, column):
        return (grp, (row * 2 + column) * 2 + core)

    mate = (grp, me + 1 - 2 * core)
    across = (grp + 1 - 2 * side, me)
    beside = at(line, 1 - y)
    half = lines // 2
    high = line // half
    low = high * half
    inside = [low + (line + i) % half for i in range(1, half)]
    crossing = [(half + i) * (1 - high) + (half - 1 - i) * high for i in range(half)]
    order = inside + crossing
    near_gate = (half - 1) * (1 - high) + half * high
    far_gate = half * (1 - high) + (half - 1) * high
    subs = 2
    part = shard // subs
    pieces = 2 * subs
    third = depth // 3 // 128 * 128
    middle = depth - 2 * third
    cols = [
        pl.ds(pl.multiple_of(side * (depth - third), 128), third),
        pl.ds(third, middle),
        pl.ds(pl.multiple_of((1 - side) * (depth - third), 128), third),
    ]

    def start(copy):
        copy.start()
        sends.append(copy)

    passed = []

    def view(chip_at, core_at, p):
        return held.at[chip_at, core_at, pl.ds(p % subs * part, part), cols[p // subs]]

    def column(j):
        return pl.ds(pl.multiple_of(j * span, span), span)

    own = pltpu.make_async_copy(w_any, held.at[chip, core], load_sems.at[0])
    own.start()
    loads = [
        pltpu.make_async_copy(src, dst, load_sems.at[1 + i])
        for i, (src, dst) in enumerate([
            (hidden_any, hidden), (in_re_any, in_re), (in_im_any, in_im), (out_re_any, out_re), (out_im_any, out_im),
            (w_glu_any, glu_w), (w_out_any, out_w),
        ])
    ]
    for load in loads[:1]:
        load.start()
    meet([at(o, y) for o in order] + [beside, mate, across])
    own.wait()
    for p in range(pieces):
        spot = view(chip, core, p)
        start(remote(spot, spot, ys.at[line, p], yr.at[line, p], beside))
        for o in inside + [far_gate]:
            start(remote(spot, spot, zs.at[o, p], zr.at[line, p], at(o, y)))
    spot = held.at[chip, core]
    start(remote(spot, spot, own_s, own_r, mate))
    for load in loads[1:]:
        load.start()
    block_loads = [
        pltpu.make_async_copy(state_any.at[:, :, pl.ds(j * span, span)], state.at[:, :, pl.ds(j * span, span)], state_sems.at[j])
        for j in range(blocks)
    ]
    for load in block_loads + expert_loads:
        load.start()

    def iota(shape, axis):
        return lax.broadcasted_iota(jnp.int32, shape, axis)

    loads[0].wait()
    wide = hidden[...].astype(F32)
    mean = jnp.mean(wide * wide, axis=-1, keepdims=True)
    normed[...] = (wide * lax.rsqrt(mean + 1e-06) * gain_ref[...]).astype(BF16)

    groups = lam_re_ref.shape[0]
    lr, li = lam_re_ref[...], lam_im_ref[...]
    diagonal = iota((groups, groups), 0) == iota((groups, groups), 1)
    step = jnp.exp(jnp.sum(jnp.where(diagonal, step_ref[...], 0.0), axis=1, keepdims=True))
    magnitude = jnp.exp(lr * step)
    bar_re = magnitude * jnp.cos(li * step)
    bar_im = magnitude * jnp.sin(li * step)
    denom = lr * lr + li * li
    lessened = bar_re - 1.0
    coef[0] = bar_re
    coef[1] = bar_im
    coef[2] = (lessened * lr + bar_im * li) / denom
    coef[3] = (bar_im * lr - lessened * li) / denom
    for load in loads[1:5]:
        load.wait()
    for load in block_loads:
        load.wait()
    gating[...] = jnp.zeros_like(gating)

    spread = iota((entries, span), 1) % entries == iota((entries, span), 0)
    mask = iota((128, span), 0) // channels == iota((128, span), 1) // entries
    pick = iota((span // entries, span), 0) == iota((span // entries, span), 1) // entries

    def expand(ref, j):
        part = ref[pl.ds(pl.multiple_of(j * 128, 128), 128), :].astype(BF16)
        tiled = jnp.dot(part, spread.astype(BF16), preferred_element_type=F32)
        return jnp.where(mask, tiled, 0.0).astype(BF16)

    def mix(j):
        block = held[pl.ds(j * unit, unit)].reshape(128, depth)
        inputs = lax.dot_general(normed[...], block, NT, preferred_element_type=F32).astype(BF16)
        drive_re = jnp.dot(inputs, expand(in_re, j), preferred_element_type=F32)
        drive_im = jnp.dot(inputs, expand(in_im, j), preferred_element_type=F32)
        per = span // entries
        rows = coef[:, pl.ds(pl.multiple_of(j * per, per), per), :].reshape(4 * per, entries)
        tiled = jnp.dot(rows, spread.astype(F32), precision=lax.Precision.HIGHEST, preferred_element_type=F32)
        line_of = [
            jnp.sum(jnp.where(pick, tiled[i * per : (i + 1) * per], 0.0), axis=0, keepdims=True) for i in range(4)
        ]
        old_re, old_im = state[0, :, column(j)], state[1, :, column(j)]
        new_re = line_of[0] * old_re - line_of[1] * old_im + (line_of[2] * drive_re - line_of[3] * drive_im)
        new_im = line_of[0] * old_im + line_of[1] * old_re + (line_of[2] * drive_im + line_of[3] * drive_re)
        state[0, :, column(j)] = new_re
        state[1, :, column(j)] = new_im
        read = lax.dot_general(new_re.astype(BF16), expand(out_re, j), NT, preferred_element_type=F32)
        read = read - lax.dot_general(new_im.astype(BF16), expand(out_im, j), NT, preferred_element_type=F32)
        lanes = pl.ds(pl.multiple_of(j * 128, 128), 128)
        act = jax.nn.gelu(read + skip_ref[:, lanes] * inputs.astype(F32))
        active[:, lanes] = act
        gating[...] += jnp.dot(act.astype(BF16), glu_w[lanes, :], preferred_element_type=F32)

    def place(item):
        kind, k = item
        if kind == 0:
            return order[k] * 2 + y
        return (line if k < 0 else order[k]) * 2 + 1 - y

    def forward(k, p, spot):
        s = order[k]
        copies = [
            remote(spot, spot, fs.at[k - half + 1, p, i], zr.at[s, p], at(target, y)) for i, target in enumerate(inside)
        ]
        passed.extend(copies)

        @pl.when(line == near_gate)
        def _():
            for copy in copies:
                copy.start()

    def take(item, p):
        kind, k = item
        s = line if k < 0 else order[k]
        spot = view(place(item), core, p)
        if kind == 0:
            remote(spot, spot, zs.at[s, p], zr.at[s, p], mate).wait_recv()
            if k >= half - 1:
                forward(k, p, spot)
            start(remote(spot, spot, ys.at[s, p], yr.at[s, p], beside))
        else:
            remote(spot, spot, ys.at[s, p], yr.at[s, p], mate).wait_recv()
        if p < subs:
            start(remote(spot, spot, xs.at[place(item), p], xr.at[place(item), p], across))
        start(remote(spot, spot, ds.at[place(item), p], dr.at[place(item), p], mate))

    def take_x(item, u):
        spot = view(place(item), core, pieces + u)
        remote(spot, spot, xs.at[place(item), u], xr.at[place(item), u], mate).wait_recv()
        start(remote(spot, spot, ds.at[place(item), pieces + u], dr.at[place(item), pieces + u], mate))

    ready = {-1: 1}

    def finish(item):
        for p in range(pieces + subs):
            spot = view(place(item), 1 - core, p)
            remote(spot, spot, ds.at[place(item), p], dr.at[place(item), p], mate).wait_recv()
        if unit == 1:
            mix(place(item))
        else:
            k = item[1]
            ready[k] = ready.get(k, 0) + 1
            if ready[k] == unit:
                mix(line if k < 0 else order[k])

    names = {"o": (1, -1), "a": (0, 0), "b": (0, 1), "c": (0, 2), "A": (1, 0), "B": (1, 1), "C": (1, 2)}
    if lines == 4:
        plan = [(names[word[0]], word[1]) for word in words(GATHER_ORDER)]
    else:
        items = [(1, -1)]
        for k in range(lines):
            if k < lines - 1:
                items.append((0, k))
            if k > 0:
                items.append((1, k - 1))
        plan = [(item, str(p)) for p in range(pieces) for item in items]
        plan += [(item, step) for item in items for step in [str(pieces + u) for u in range(subs)] + ["m"]]
    spot = held.at[chip, 1 - core]
    remote(spot, spot, own_s, own_r, mate).wait_recv()
    loads[5].wait()
    if unit == 1:
        mix(chip)
    for item, step in plan:
        if step == "m":
            finish(item)
        elif int(step) < pieces:
            take(item, int(step))
        else:
            take_x(item, int(step) - pieces)
    loads[6].wait()

    act = active[...]
    glu = (act * jax.nn.sigmoid(gating[...])).astype(BF16)
    resid = (hidden[...].astype(F32) + jnp.dot(glu, out_w[...], preferred_element_type=F32)).astype(BF16)
    resid_ref[...] = resid
    wide = resid.astype(F32)
    mean = jnp.mean(wide * wide, axis=-1, keepdims=True)
    second_normed = (wide * lax.rsqrt(mean + 1e-06) * ffn_gain_ref[...]).astype(BF16)
    rows_ref[:, :depth] = second_normed
    level = lax.dot_general(second_normed, w_group_ref[...], NT, preferred_element_type=F32)
    logits = lax.dot_general(second_normed, w_route_ref[...], NT, preferred_element_type=F32)
    count = second_normed.shape[0]
    lane = iota((count, 128), 1)
    same = (iota((count, count), 0) == iota((count, count), 1)).astype(BF16)
    ids = lax.dot_general(same, ids_ref[...].astype(F32).astype(BF16), NT, preferred_element_type=F32).astype(jnp.int32)
    first, second = ids[:, 0:1], ids[:, 1:2]
    group = first // per_group
    chosen = jnp.sum(jnp.where(iota(level.shape, 1) == group, level, 0.0), axis=1, keepdims=True)
    scale = 1.0 / jnp.sum(jnp.exp(level - chosen), axis=1, keepdims=True)
    r0 = jnp.sum(jnp.where(iota(logits.shape, 1) == first, logits, 0.0), axis=1, keepdims=True)
    r1 = jnp.sum(jnp.where(iota(logits.shape, 1) == second, logits, 0.0), axis=1, keepdims=True)
    share = jax.nn.sigmoid(r0 - r1)
    member = lane % per_group
    gate = jnp.where(member == first % per_group, scale * share, 0.0)
    gate = gate + jnp.where(member == second % per_group, scale * (1.0 - share), 0.0)
    high = gate.astype(BF16).astype(F32)
    packed = jnp.where(lane < per_group, high, jnp.where(lane < 2 * per_group, gate - high, 0.0))
    rows_ref[:, depth:] = packed.astype(BF16)
    hits = (lane == group).astype(BF16)
    earlier = (iota((count, count), 1) < iota((count, count), 0)).astype(BF16)
    before = jnp.dot(earlier, hits, preferred_element_type=F32)
    rank = jnp.sum(jnp.where(lane == group, before, 0.0), axis=1, keepdims=True).astype(jnp.int32)
    slots = place_ref.shape[1]
    slot = group * (slots // EXP_GROUPS) + rank
    place_ref[...] = (iota((count, slots), 1) == slot).astype(BF16)

    @pl.when(line == near_gate)
    def _():
        for copy in passed:
            copy.wait_send()


def experts(
    groups, per_group, subs, chunks, sends, rows_ref, place_ref, returned,
    outgoing, tokens, parts, parts_in, sums, sums_in, final, w_gate, w_up, w_down,
    zs, zr, ys, yr, cs, cr, ps, pr, qs, qr, bs, br, loads,
):
    grp = lax.axis_index("grp")
    me = lax.axis_index("ep")
    pairs = per_group // 2
    g, p = me // per_group, me % per_group
    q, c = p // 2, p % 2
    depth = returned.shape[2]
    cap = outgoing.shape[1]
    wide = outgoing.shape[2]
    part = cap // subs
    spans = [pl.ds(i * part, part) for i in range(subs)]

    def at(group, pair):
        return (grp, group * per_group + pair * 2 + c)

    mate = (grp, me + 1 - 2 * c)
    half = groups // 2
    low = g // half * half
    crossing = [(low + half) % groups + (g + i) % half for i in range(half)]
    inside = [low + (g + i) % half for i in range(1, half)]
    sources = [g] + inside + crossing
    others = sources[1:]
    mates_q = [(q + j) % pairs for j in range(1, pairs)]
    sent = lax.dot_general(place_ref[...], rows_ref[...], TN, preferred_element_type=F32).astype(BF16)
    outgoing[...] = sent.reshape(groups, cap, wide)
    tokens[g, c, q] = outgoing[g]

    def start(copy):
        copy.start()
        sends.append(copy)

    for word in words(SEND_ORDER):
        target, u = sources[int(word[0])], int(word[1])
        start(remote(
            outgoing.at[target, spans[u]], tokens.at[g, c, q, spans[u]], zs.at[target, u], zr.at[g, u], at(target, q)
        ))

    def spread(k, u):
        s = sources[k]
        spot = tokens.at[s, c, q, spans[u]]
        if k > 0:
            remote(spot, spot, zs.at[s, u], zr.at[s, u], mate).wait_recv()
        for o in mates_q:
            start(remote(spot, spot, ys.at[s, o, u], yr.at[s, q, u], at(g, o)))
        start(remote(spot, spot, cs.at[s, q, u], cr.at[s, q, u], mate))

    def relay(k, u):
        s = sources[k]
        for o in mates_q:
            spot = tokens.at[s, c, o, spans[u]]
            remote(spot, spot, ys.at[s, o, u], yr.at[s, o, u], mate).wait_recv()
            start(remote(spot, spot, cs.at[s, o, u], cr.at[s, o, u], mate))

    fold = subs // chunks
    bulk = cap // chunks

    def inner_rows(u):
        return pl.ds(u % fold * part, part)

    def compute(k, h):
        s = sources[k]
        for u in range(h * fold, h * fold + fold):
            for o in range(pairs):
                spot = tokens.at[s, 1 - c, o, spans[u]]
                remote(spot, spot, cs.at[s, o, u], cr.at[s, o, u], mate).wait_recv()
        if not loaded:
            loaded.append(True)
            for load in loads:
                load.wait()
        total = per_group * bulk
        x = tokens[s, :, :, pl.ds(h * bulk, bulk)].reshape(total, wide)
        rows = x[:, :depth]
        gate = jnp.dot(rows, w_gate[...], preferred_element_type=F32)
        upper = jnp.dot(rows, w_up[...], preferred_element_type=F32)
        inner = (jax.nn.silu(gate) * upper).astype(BF16)
        result = jnp.dot(inner, w_down[...], preferred_element_type=F32).astype(BF16)
        lane = lax.broadcasted_iota(jnp.int32, (total, wide - depth), 1)
        mine = (lane == p) | (lane == p + per_group)
        weight = jnp.sum(jnp.where(mine, x[:, depth:].astype(F32), 0.0), axis=1, keepdims=True)
        parts[s, h] = (result.astype(F32) * weight).astype(BF16).reshape(2, pairs, bulk, depth)
        start(remote(parts.at[s, h, 1 - c], parts_in.at[s, h], ps.at[s, h], pr.at[s, h], mate))

    loaded = []
    merged = set()

    def reduce_mate(k, u):
        s, h = sources[k], u // fold
        if (k, h) not in merged:
            merged.add((k, h))
            spot = parts_in.at[s, h]
            remote(spot, spot, ps.at[s, h], pr.at[s, h], mate).wait_recv()
        sums[s, u] = (
            parts[s, h, c, :, inner_rows(u)].astype(F32) + parts_in[s, h, :, inner_rows(u)].astype(F32)
        ).astype(BF16)
        for o in mates_q:
            start(remote(sums.at[s, u, o], sums_in.at[s, u, q], qs.at[s, o, u], qr.at[s, q, u], at(g, o)))

    def reduce_pairs(k, u):
        s = sources[k]
        total = sums[s, u, q].astype(F32)
        for o in mates_q:
            spot = sums_in.at[s, u, o]
            remote(spot, spot, qs.at[s, o, u], qr.at[s, o, u], mate).wait_recv()
            total = total + sums_in[s, u, o].astype(F32)
        if k == 0:
            returned[g, spans[u]] = total.astype(BF16)
        else:
            final[s, spans[u]] = total.astype(BF16)
            start(remote(
                final.at[s, spans[u]], returned.at[g, spans[u]], bs.at[s, u], br.at[g, u], at(s, q)
            ))

    stages = {"F": spread, "G": relay, "C": compute, "M": reduce_mate, "E": reduce_pairs}
    for word in words(EXPERT_ORDER):
        stages[word[0]](int(word[1]), int(word[2]))
    for o in others:
        for u in range(subs):
            spot = returned.at[o, spans[u]]
            remote(spot, spot, bs.at[o, u], br.at[o, u], mate).wait_recv()


def layer_kernel(
    chips, groups, per_group, subs, chunks, *refs,
):
    inputs, outputs, scratch = refs[:21], refs[21:25], refs[25:]
    weights = inputs[18:]
    state, resid_ref, place_ref, returned = outputs
    rows_ref, *rest = scratch
    front_scratch, rest = rest[:12], rest[12:]
    front_sems, rest = rest[:13], rest[13:]
    expert_scratch, expert_sems = rest[:10], rest[10:]
    loads = [
        pltpu.make_async_copy(src.at[0], dst, expert_sems[-1].at[i])
        for i, (src, dst) in enumerate(zip(weights, expert_scratch[7:]))
    ]
    sends = []

    def meet(peers):
        grp = lax.axis_index("grp")
        me = lax.axis_index("ep")
        g, p = me // per_group, me % per_group
        ahead = [(grp, (g + i) % groups * per_group + p) for i in range(1, groups)]
        near = [(grp, g * per_group + (p + 2 * i) % per_group) for i in range(1, per_group // 2)]
        greet(peers + ahead + near)

    front(
        chips, per_group, sends, *inputs[:18], state, resid_ref, place_ref, rows_ref, *front_scratch, *front_sems,
        meet, loads,
    )
    experts(
        groups, per_group, subs, chunks, sends, rows_ref, place_ref, returned, *expert_scratch, *expert_sems[:-1], loads,
    )
    for copy in sends:
        copy.wait_send()


def finish_kernel(state_ref, resid_ref, place_ref, returned_ref, new_any, out_ref, sems):
    copies = [
        pltpu.make_async_copy(
            state_ref.at[i, pl.ds(j * 64, 64)], new_any.at[i, pl.ds(j * 64, 64)], sems.at[i, j]
        )
        for i in range(2) for j in range(state_ref.shape[1] // 64)
    ]
    for copy in copies:
        copy.start()
    back = returned_ref[...].reshape(-1, returned_ref.shape[2])
    moe = jnp.dot(place_ref[...], back, preferred_element_type=F32)
    out_ref[...] = (resid_ref[...].astype(F32) + moe).astype(BF16)
    for copy in copies:
        copy.wait()


def on_device(
    hidden, state, norm_gain, w_in, lam_re, lam_im, log_step, in_re, in_im, out_re, out_im, skip, w_glu, w_out,
    ffn_gain, w_group, w_route, w_gate, w_up, w_down, route_ids,
):
    rows, depth = hidden.shape
    devices = lax.axis_size("ep")
    chips = devices // 2
    shard = w_in.shape[1]
    dma = pltpu.SemaphoreType.DMA
    groups, entries = lam_re.shape
    width = in_re.shape[2]
    channels = groups * width
    lines = chips // 2
    blocks = channels // 128
    experts = w_route.shape[1]
    per_group = experts // EXP_GROUPS
    cap = 2 * rows // EXP_GROUPS
    pairs = per_group // 2
    G = EXP_GROUPS
    subs, chunks = 4, 2
    part, bulk = cap // subs, cap // chunks
    vm = pltpu.VMEM
    kept = [
        vm(state.shape, F32), vm((rows, depth), BF16), vm((rows, G * cap), BF16), vm((G, cap, depth), BF16),
    ]
    results = pl.pallas_call(
        functools.partial(layer_kernel, chips, G, per_group, subs, chunks),
        out_shape=kept,
        in_specs=[ANY, VMEM, ANY, ANY] + [VMEM] * 3 + [ANY] * 4 + [VMEM] * 2 + [ANY] * 2 + [VMEM] * 3 + [ANY] * 3,
        out_specs=[VMEM] * 4,
        scratch_shapes=[
            vm((rows, depth + 128), BF16),
            vm((chips, 2, shard, depth), BF16),
            vm((rows, depth), BF16),
        ] + [vm((channels, entries), F32)] * 4 + [
            vm(w_glu.shape, BF16),
            vm(w_out.shape, BF16),
            vm((rows, depth), BF16),
            vm((4, groups, entries), F32),
            vm((rows, channels), F32),
            vm((rows, channels), F32),
        ] + [dma((lines, 4))] * 4 + [dma((chips, 2))] * 2 + [dma((chips, 6))] * 2
        + [dma((lines // 2, 4, lines // 2 - 1)), dma, dma, dma((8,)), dma((blocks,))] + [
            vm((G, cap, depth + 128), BF16),
            vm((G, 2, pairs, cap, depth + 128), BF16),
            vm((G, chunks, 2, pairs, bulk, depth), BF16),
            vm((G, chunks, pairs, bulk, depth), BF16),
            vm((G, subs, pairs, part, depth), BF16),
            vm((G, subs, pairs, part, depth), BF16),
            vm((G, cap, depth), BF16),
            vm(w_gate.shape[1:], BF16),
            vm(w_up.shape[1:], BF16),
            vm(w_down.shape[1:], BF16),
        ] + [dma((G, subs))] * 2 + [dma((G, pairs, subs))] * 4 + [dma((G, chunks))] * 2 + [dma((G, pairs, subs))] * 2
        + [dma((G, subs))] * 2 + [dma((3,))],
        compiler_params=pltpu.CompilerParams(collective_id=0, has_side_effects=True, vmem_limit_bytes=LIMIT),
        name="layer",
    )(
        hidden, norm_gain[None, :], w_in.T, state, lam_re, lam_im, log_step[None, :],
        in_re.transpose(0, 2, 1).reshape(channels, entries), in_im.transpose(0, 2, 1).reshape(channels, entries),
        out_re.reshape(channels, entries), out_im.reshape(channels, entries), skip[None, :], ffn_gain[None, :],
        w_glu, w_out, w_group.T, w_route.T, route_ids.T, w_gate, w_up, w_down,
    )
    new_state, hidden_out = pl.pallas_call(
        finish_kernel,
        out_shape=[jax.ShapeDtypeStruct(state.shape, F32), jax.ShapeDtypeStruct((rows, depth), BF16)],
        in_specs=[VMEM] * 4,
        out_specs=[ANY, VMEM],
        scratch_shapes=[dma((2, rows // 64))],
        compiler_params=pltpu.CompilerParams(vmem_limit_bytes=FINISH_LIMIT),
        name="finish",
    )(*results)
    return (hidden_out, new_state)


def solution(mesh):
    return jax.shard_map(
        on_device,
        mesh=mesh,
        in_specs=(
            P(("grp", "ep"), None),
            P(None, ("grp", "ep"), None),
            P(),
            P(None, "ep"),
            P(),
            P(),
            P(),
            P(),
            P(),
            P(),
            P(),
            P(),
            P(),
            P(),
            P(),
            P(),
            P(),
            P("ep", None, None),
            P("ep", None, None),
            P("ep", None, None),
            P(("grp", "ep"), None),
        ),
        out_specs=(P(("grp", "ep"), None), P(None, ("grp", "ep"), None)),
        check_vma=False,
    )
```

```python
import functools

import jax
import jax.numpy as jnp
from jax import lax
from jax.experimental import pallas as pl
from jax.experimental.pallas import tpu as pltpu
from jax.sharding import PartitionSpec as P

EXP_GROUPS = 4
TOPK = 2
MESH = pl.DeviceIdType.MESH
VMEM = pl.BlockSpec(memory_space=pltpu.VMEM)
ANY = pl.BlockSpec(memory_space=pl.ANY)
F32 = jnp.float32
BF16 = jnp.bfloat16
NT = (((1,), (1,)), ((), ()))
TN = (((0,), (0,)), ((), ()))
GATHER_ORDER = (
    "p o0 a0 w", "o1 a1 o2 b0", "c0 o4 b1 a4", "c1 A1 o3 o5", "a2 A0 a5 B0", "a3 b2 om c2",
    "am b3 B1 b4", "b5 C1 C0 A2", "c5 c4 c3 A5", "bm B2 A3 A4", "cm C2 B5 B4", "C5 B3 Am C4",
    "C3 Bm Cm",
)
SEND_ORDER = (
    "20 10 30 11", "21 13 31 12", "22 32 23 33",
)
EXPERT_ORDER = (
    "F00 F01 F02 F20", "G00 F03 G01 F10", "C00 F30 G03 G02", "F21 G20 F11 F13", "C01 G21 F31 F12", "G10 G30 C20 G11",
    "G13 F22 G31 M21", "M20 C30 F23 F32", "C10 E20 M30 E21", "G22 G23 M10 G12", "F33 M31 M11 C21", "G32 E30 C11 G33",
    "M22 M23 E31 E10", "M12 C31 E22 E11", "M02 M32 E23 M13", "M33 E12 E32 M01", "M03 E13 M00 E33", "E01 E03 E02 E00",
)
LIMIT = 57 * 1024 * 1024
FINISH_LIMIT = 16 * 1024 * 1024


def remote(src, dst, send_sem, recv_sem, device):
    return pltpu.make_async_remote_copy(
        src_ref=src, dst_ref=dst, send_sem=send_sem, recv_sem=recv_sem, device_id=device, device_id_type=MESH
    )


def greet(peers):
    barrier = pltpu.get_barrier_semaphore()
    for peer in peers:
        pl.semaphore_signal(barrier, inc=1, device_id=peer, device_id_type=MESH)
    pl.semaphore_wait(barrier, len(peers))


def words(table):
    return [word for text in table for word in text.split()]


def front(
    chips, per_group, sends, hidden_any, gain_any, w_any, state_any, lam_re_any, lam_im_any, step_any, in_re_any, in_im_any,
    out_re_any, out_im_any, skip_any, ffn_gain_any, w_glu_any, w_out_any, w_group_any, w_route_any, ids_any,
    state, resid_ref, place_ref, rows_ref, shares_ref, picks,
    held, hidden, in_re, in_im, out_re, out_im, glu_w, out_w, normed, coef, active, strips, into, outof, rounded,
    gain_ref, lam_re_ref, lam_im_ref, step_ref, skip_ref, ffn_gain_ref, w_group_ref, w_route_ref, ids_ref,
    zs, zr, ys, yr, xs, xr, ds, dr, fs, own_s, own_r, load_sems, state_sems, meet, expert_loads,
):
    grp = lax.axis_index("grp")
    me = lax.axis_index("ep")
    chip, core = me // 2, me % 2
    lines = chips // 2
    line, y = chip // 2, chip % 2
    side = grp % 2
    shard, depth = w_any.shape
    entries = lam_re_any.shape[1]
    unit = 128 // (2 * shard)
    blocks = chips // unit
    span = state.shape[2] // blocks
    channels = 128 // (span // entries)

    def at(row, column):
        return (grp, (row * 2 + column) * 2 + core)

    mate = (grp, me + 1 - 2 * core)
    across = (grp + 1 - 2 * side, me)
    beside = at(line, 1 - y)
    half = lines // 2
    high = line // half
    low = high * half
    inside = [low + (line + i) % half for i in range(1, half)]
    crossing = [(half + i) * (1 - high) + (half - 1 - i) * high for i in range(half)]
    order = inside + crossing
    near_gate = (half - 1) * (1 - high) + half * high
    far_gate = half * (1 - high) + (half - 1) * high
    subs = 2
    part = shard // subs
    pieces = 2 * subs
    third = depth // 3 // 128 * 128
    middle = depth - 2 * third
    cols = [
        pl.ds(pl.multiple_of(side * (depth - third), 128), third),
        pl.ds(third, middle),
        pl.ds(pl.multiple_of((1 - side) * (depth - third), 128), third),
    ]

    def start(copy):
        copy.start()
        sends.append(copy)

    passed = []

    def view(chip_at, core_at, p):
        return held.at[chip_at, core_at, pl.ds(p % subs * part, part), cols[p // subs]]

    def column(j):
        return pl.ds(pl.multiple_of(j * span, span), span)

    own = pltpu.make_async_copy(w_any, held.at[chip, core], load_sems.at[0])
    own.start()
    loads = [
        pltpu.make_async_copy(src, dst, load_sems.at[1 + i])
        for i, (src, dst) in enumerate([
            (hidden_any, hidden), (in_re_any, in_re), (in_im_any, in_im), (out_re_any, out_re), (out_im_any, out_im),
            (w_glu_any, glu_w), (w_out_any, out_w), (gain_any, gain_ref), (lam_re_any, lam_re_ref), (lam_im_any, lam_im_ref),
            (step_any, step_ref), (skip_any, skip_ref), (ffn_gain_any, ffn_gain_ref), (w_group_any, w_group_ref),
            (w_route_any, w_route_ref), (ids_any, ids_ref),
        ])
    ]
    block_loads = [
        pltpu.make_async_copy(state_any.at[:, :, pl.ds(j * span, span)], state.at[:, :, pl.ds(j * span, span)], state_sems.at[j])
        for j in range(blocks)
    ]
    for load in loads[:1] + loads[7:] + loads[1:5] + block_loads + loads[5:7] + expert_loads:
        load.start()
    meet([at(o, y) for o in order] + [beside, mate, across])
    own.wait()
    for p in range(pieces):
        spot = view(chip, core, p)
        start(remote(spot, spot, ys.at[line, p], yr.at[line, p], beside))
        for o in inside + [far_gate]:
            start(remote(spot, spot, zs.at[o, p], zr.at[line, p], at(o, y)))
    spot = held.at[chip, core]
    start(remote(spot, spot, own_s, own_r, mate))

    def iota(shape, axis):
        return lax.broadcasted_iota(jnp.int32, shape, axis)

    def prepare():
        for load in loads[:5] + loads[7:] + block_loads:
            load.wait()
        prepare_all()

    tiles = span // 128
    stack = tiles * blocks

    def twin(value):
        return jnp.concatenate([value] * (128 // entries), axis=1)

    def prepare_all():
        wide = hidden[...].astype(F32)
        mean = jnp.mean(wide * wide, axis=-1, keepdims=True)
        normed[...] = (wide * lax.rsqrt(mean + 1e-06) * gain_ref[...]).astype(BF16)

        groups = lam_re_ref.shape[0]
        lr, li = lam_re_ref[...], lam_im_ref[...]
        diagonal = iota((groups, groups), 0) == iota((groups, groups), 1)
        step = jnp.exp(jnp.sum(jnp.where(diagonal, step_ref[...], 0.0), axis=1, keepdims=True))
        magnitude = jnp.exp(lr * step)
        bar_re = magnitude * jnp.cos(li * step)
        bar_im = magnitude * jnp.sin(li * step)
        denom = lr * lr + li * li
        lessened = bar_re - 1.0
        first_half = iota((stack, 128), 1) < entries
        for i, value in enumerate([
            bar_re, bar_im, (lessened * lr + bar_im * li) / denom, (bar_im * lr - lessened * li) / denom,
        ]):
            coef[i] = twin(value)
            even, odd = coef[i, pl.ds(0, stack, stride=2), :], coef[i, pl.ds(1, stack, stride=2), :]
            chosen = jnp.where(first_half, even, odd)
            for j in range(blocks):
                strips[i, j] = chosen[j * tiles : (j + 1) * tiles]
        into[...] = jnp.zeros_like(into)
        outof[...] = jnp.zeros_like(outof)

        count = hidden.shape[0]
        lane = iota((count, 128), 1)
        same = (iota((count, count), 0) == iota((count, count), 1)).astype(BF16)
        ids = lax.dot_general(same, ids_ref[...].astype(F32).astype(BF16), NT, preferred_element_type=F32).astype(jnp.int32)
        group = ids[:, 0:1] // per_group
        hits = (lane == group).astype(BF16)
        earlier = (iota((count, count), 1) < iota((count, count), 0)).astype(BF16)
        before = jnp.dot(earlier, hits, preferred_element_type=F32)
        rank = jnp.sum(jnp.where(lane == group, before, 0.0), axis=1, keepdims=True).astype(jnp.int32)
        slots = place_ref.shape[1]
        slot = group * (slots // EXP_GROUPS) + rank
        place_ref[...] = (iota((count, slots), 1) == slot).astype(BF16)
        picks[...] = jnp.where(lane == 0, ids[:, 0:1], ids[:, 1:2])

    rise = 128 // tiles
    inside_tile = iota((128, 128), 0) // channels % 2 == iota((128, 128), 1) // entries

    def expand(ref, j, target, base, sign):
        part_of = ref[pl.ds(pl.multiple_of(j * 128, 128), 128), :]
        tile = jnp.where(inside_tile, twin(part_of), 0.0)
        tile = (tile if sign > 0 else -tile).astype(BF16)
        for t in range(tiles):
            target[t * rise : (t + 1) * rise, base + t * 128 : base + (t + 1) * 128] = tile[t * rise : (t + 1) * rise]

    def mix(j):
        expand(in_re, j, into, 0, 1)
        expand(in_im, j, into, span, 1)
        expand(out_re, j, outof, 0, 1)
        expand(out_im, j, outof, span, -1)
        block = held[pl.ds(j * unit, unit)].reshape(128, depth)
        inputs = lax.dot_general(normed[...], block, NT, preferred_element_type=F32).astype(BF16)
        drive = jnp.dot(inputs, into[...], preferred_element_type=F32)
        strip = [strips[i, j] for i in range(4)]
        for t in range(tiles):
            lanes = pl.ds(pl.multiple_of(j * span + t * 128, 128), 128)
            row = [value[t : t + 1] for value in strip]
            drive_re = drive[:, t * 128 : (t + 1) * 128]
            drive_im = drive[:, span + t * 128 : span + (t + 1) * 128]
            old_re, old_im = state[0, :, lanes], state[1, :, lanes]
            new_re = row[0] * old_re - row[1] * old_im + (row[2] * drive_re - row[3] * drive_im)
            new_im = row[0] * old_im + row[1] * old_re + (row[2] * drive_im + row[3] * drive_re)
            state[0, :, lanes] = new_re
            state[1, :, lanes] = new_im
            rounded[:, t * 128 : (t + 1) * 128] = new_re.astype(BF16)
            rounded[:, span + t * 128 : span + (t + 1) * 128] = new_im.astype(BF16)
        read = lax.dot_general(rounded[...], outof[...], NT, preferred_element_type=F32)
        lanes = pl.ds(pl.multiple_of(j * 128, 128), 128)
        act = jax.nn.gelu(read + skip_ref[:, lanes] * inputs.astype(F32))
        active[:, lanes] = act

    def place(item):
        kind, k = item
        if kind == 0:
            return order[k] * 2 + y
        return (line if k < 0 else order[k]) * 2 + 1 - y

    def forward(k, p, spot):
        s = order[k]
        copies = [
            remote(spot, spot, fs.at[k - half + 1, p, i], zr.at[s, p], at(target, y)) for i, target in enumerate(inside)
        ]
        passed.extend(copies)

        @pl.when(line == near_gate)
        def _():
            for copy in copies:
                copy.start()

    def take(item, p):
        kind, k = item
        s = line if k < 0 else order[k]
        spot = view(place(item), core, p)
        if kind == 0:
            remote(spot, spot, zs.at[s, p], zr.at[s, p], mate).wait_recv()
            if k >= half - 1:
                forward(k, p, spot)
            start(remote(spot, spot, ys.at[s, p], yr.at[s, p], beside))
        else:
            remote(spot, spot, ys.at[s, p], yr.at[s, p], mate).wait_recv()
        if p < subs:
            start(remote(spot, spot, xs.at[place(item), p], xr.at[place(item), p], across))
        start(remote(spot, spot, ds.at[place(item), p], dr.at[place(item), p], mate))

    def take_x(item, u):
        spot = view(place(item), core, pieces + u)
        remote(spot, spot, xs.at[place(item), u], xr.at[place(item), u], mate).wait_recv()
        start(remote(spot, spot, ds.at[place(item), pieces + u], dr.at[place(item), pieces + u], mate))

    ready = {-1: 1}

    def finish(item):
        for p in range(pieces + subs):
            spot = view(place(item), 1 - core, p)
            remote(spot, spot, ds.at[place(item), p], dr.at[place(item), p], mate).wait_recv()
        if unit == 1:
            mix(place(item))
        else:
            k = item[1]
            ready[k] = ready.get(k, 0) + 1
            if ready[k] == unit:
                mix(line if k < 0 else order[k])

    names = {"o": (1, -1), "a": (0, 0), "b": (0, 1), "c": (0, 2), "A": (1, 0), "B": (1, 1), "C": (1, 2)}
    if lines == 4:
        plan = [(names.get(word[0]), word[-1]) for word in words(GATHER_ORDER)]
    else:
        items = [(1, -1)]
        for k in range(lines):
            if k < lines - 1:
                items.append((0, k))
            if k > 0:
                items.append((1, k - 1))
        plan = [(None, "p"), (None, "w")] + [(item, str(p)) for p in range(pieces) for item in items]
        plan += [(item, step) for item in items for step in [str(pieces + u) for u in range(subs)] + ["m"]]
    for item, step in plan:
        if step == "p":
            prepare()
        elif step == "w":
            spot = held.at[chip, 1 - core]
            remote(spot, spot, own_s, own_r, mate).wait_recv()
            if unit == 1:
                mix(chip)
        elif step == "m":
            finish(item)
        elif int(step) < pieces:
            take(item, int(step))
        else:
            take_x(item, int(step) - pieces)
    loads[5].wait()
    loads[6].wait()

    act = active[...]
    gating = jnp.dot(act.astype(BF16), glu_w[...], preferred_element_type=F32)
    glu = (act * jax.nn.sigmoid(gating)).astype(BF16)
    resid = (hidden[...].astype(F32) + jnp.dot(glu, out_w[...], preferred_element_type=F32)).astype(BF16)
    resid_ref[...] = resid
    wide = resid.astype(F32)
    mean = jnp.mean(wide * wide, axis=-1, keepdims=True)
    second_normed = (wide * lax.rsqrt(mean + 1e-06) * ffn_gain_ref[...]).astype(BF16)
    rows_ref[...] = second_normed

    def share_out():
        level = lax.dot_general(rows_ref[...], w_group_ref[...], NT, preferred_element_type=F32)
        logits = lax.dot_general(rows_ref[...], w_route_ref[...], NT, preferred_element_type=F32)
        first, second = picks[:, 0:1], picks[:, 1:2]
        lane = iota(picks.shape, 1)
        group = first // per_group
        chosen = jnp.sum(jnp.where(iota(level.shape, 1) == group, level, 0.0), axis=1, keepdims=True)
        scale = 1.0 / jnp.sum(jnp.exp(level - chosen), axis=1, keepdims=True)
        r0 = jnp.sum(jnp.where(iota(logits.shape, 1) == first, logits, 0.0), axis=1, keepdims=True)
        r1 = jnp.sum(jnp.where(iota(logits.shape, 1) == second, logits, 0.0), axis=1, keepdims=True)
        share = jax.nn.sigmoid(r0 - r1)
        member = lane % per_group
        gate = jnp.where(member == first % per_group, scale * share, 0.0)
        gate = gate + jnp.where(member == second % per_group, scale * (1.0 - share), 0.0)
        high = gate.astype(BF16).astype(F32)
        low_lanes = (lane >= 8) & (lane < 8 + per_group)
        shares_ref[...] = jnp.where(lane < per_group, high, jnp.where(low_lanes, gate - high, 0.0)).astype(BF16)
        return lax.dot_general(shares_ref[...], place_ref[...], TN, preferred_element_type=F32)

    @pl.when(line == near_gate)
    def _():
        for copy in passed:
            copy.wait_send()
    return share_out


def experts(
    groups, per_group, subs, chunks, sends, rows_ref, shares_ref, place_ref, returned,
    outgoing, tokens, parts, parts_in, sums, sums_in, final, w_gate, w_up, w_down, shares, shares_in,
    zs, zr, ys, yr, cs, cr, ps, pr, qs, qr, bs, br, gs, gr, hs, hr, ks, kr, loads, share_out,
):
    grp = lax.axis_index("grp")
    me = lax.axis_index("ep")
    pairs = per_group // 2
    g, p = me // per_group, me % per_group
    q, c = p // 2, p % 2
    depth = returned.shape[2]
    cap = outgoing.shape[1]
    wide = outgoing.shape[2]
    part = cap // subs
    spans = [pl.ds(i * part, part) for i in range(subs)]

    def at(group, pair):
        return (grp, group * per_group + pair * 2 + c)

    mate = (grp, me + 1 - 2 * c)
    half = groups // 2
    low = g // half * half
    crossing = [(low + half) % groups + (g + i) % half for i in range(half)]
    inside = [low + (g + i) % half for i in range(1, half)]
    sources = [g] + inside + crossing
    others = sources[1:]
    mates_q = [(q + j) % pairs for j in range(1, pairs)]
    sent = lax.dot_general(place_ref[...], rows_ref[...], TN, preferred_element_type=F32).astype(BF16)
    outgoing[...] = sent.reshape(groups, cap, wide)
    tokens[g, c, q] = outgoing[g]
    per_tile = 128 // cap

    def start(copy):
        copy.start()
        sends.append(copy)


    def share():
        split = share_out()
        joined = split[0:8] + split[8:16]
        for i in range(groups // per_tile):
            shares[i] = joined[:, i * 128 : (i + 1) * 128]
        shares_in[g, c, q] = shares[g // per_tile]
        for target in others:
            start(remote(shares.at[target // per_tile], shares_in.at[g, c, q], gs.at[target], gr.at[g], at(target, q)))
        pass_shares(0)

    def pass_shares(k):
        s = sources[k]
        spot = shares_in.at[s, c, q]
        if k > 0:
            remote(spot, spot, gs.at[s], gr.at[s], mate).wait_recv()
        for o in mates_q:
            start(remote(spot, spot, hs.at[s, o], hr.at[s, q], at(g, o)))
        start(remote(spot, spot, ks.at[s, q], kr.at[s, q], mate))

    def dispatch(plan):
        for word in plan:
            target, u = sources[int(word[0])], int(word[1])
            start(remote(
                outgoing.at[target, spans[u]], tokens.at[g, c, q, spans[u]], zs.at[target, u], zr.at[g, u], at(target, q)
            ))

    started = {"F": set(), "G": set(), "C": set()}

    def first_of(stage, k):
        fresh = k not in started[stage]
        started[stage].add(k)
        return fresh

    def spread(k, u):
        s = sources[k]
        if first_of("F", k) and k > 0:
            pass_shares(k)
        spot = tokens.at[s, c, q, spans[u]]
        if k > 0:
            remote(spot, spot, zs.at[s, u], zr.at[s, u], mate).wait_recv()
        for o in mates_q:
            start(remote(spot, spot, ys.at[s, o, u], yr.at[s, q, u], at(g, o)))
        start(remote(spot, spot, cs.at[s, q, u], cr.at[s, q, u], mate))

    def relay(k, u):
        s = sources[k]
        if first_of("G", k):
            for o in mates_q:
                spot = shares_in.at[s, c, o]
                remote(spot, spot, hs.at[s, o], hr.at[s, o], mate).wait_recv()
                start(remote(spot, spot, ks.at[s, o], kr.at[s, o], mate))
        for o in mates_q:
            spot = tokens.at[s, c, o, spans[u]]
            remote(spot, spot, ys.at[s, o, u], yr.at[s, o, u], mate).wait_recv()
            start(remote(spot, spot, cs.at[s, o, u], cr.at[s, o, u], mate))

    fold = subs // chunks
    bulk = cap // chunks

    def inner_rows(u):
        return pl.ds(u % fold * part, part)

    spread_rows = lax.broadcasted_iota(jnp.int32, (bulk, 128), 0)
    spread_lanes = lax.broadcasted_iota(jnp.int32, (bulk, 128), 1)

    def compute(k, h):
        s = sources[k]
        if first_of("C", k):
            for o in range(pairs):
                spot = shares_in.at[s, 1 - c, o]
                remote(spot, spot, ks.at[s, o], kr.at[s, o], mate).wait_recv()
        for u in range(h * fold, h * fold + fold):
            for o in range(pairs):
                spot = tokens.at[s, 1 - c, o, spans[u]]
                remote(spot, spot, cs.at[s, o, u], cr.at[s, o, u], mate).wait_recv()
        if not loaded:
            loaded.append(True)
            for load in loads:
                load.wait()
        total = per_group * bulk
        x = tokens[s, :, :, pl.ds(h * bulk, bulk)].reshape(total, wide)
        gate = jnp.dot(x, w_gate[...], preferred_element_type=F32)
        upper = jnp.dot(x, w_up[...], preferred_element_type=F32)
        inner = (jax.nn.silu(gate) * upper).astype(BF16)
        result = jnp.dot(inner, w_down[...], preferred_element_type=F32).astype(BF16)
        own_lane = spread_lanes == spread_rows + (g % per_tile * cap + h * bulk)
        weight = jnp.concatenate([
            jnp.sum(jnp.where(own_lane, shares_in[s, i, o, pl.ds(p, 1), :], 0.0), axis=1, keepdims=True)
            for i in range(2) for o in range(pairs)
        ], axis=0)
        parts[s, h] = (result.astype(F32) * weight).astype(BF16).reshape(2, pairs, bulk, depth)
        start(remote(parts.at[s, h, 1 - c], parts_in.at[s, h], ps.at[s, h], pr.at[s, h], mate))

    loaded = []
    merged = set()

    def reduce_mate(k, u):
        s, h = sources[k], u // fold
        if (k, h) not in merged:
            merged.add((k, h))
            spot = parts_in.at[s, h]
            remote(spot, spot, ps.at[s, h], pr.at[s, h], mate).wait_recv()
        sums[s, u] = (
            parts[s, h, c, :, inner_rows(u)].astype(F32) + parts_in[s, h, :, inner_rows(u)].astype(F32)
        ).astype(BF16)
        for o in mates_q:
            start(remote(sums.at[s, u, o], sums_in.at[s, u, q], qs.at[s, o, u], qr.at[s, q, u], at(g, o)))

    def reduce_pairs(k, u):
        s = sources[k]
        total = sums[s, u, q].astype(F32)
        for o in mates_q:
            spot = sums_in.at[s, u, o]
            remote(spot, spot, qs.at[s, o, u], qr.at[s, o, u], mate).wait_recv()
            total = total + sums_in[s, u, o].astype(F32)
        if k == 0:
            returned[g, spans[u]] = total.astype(BF16)
        else:
            final[s, spans[u]] = total.astype(BF16)
            start(remote(
                final.at[s, spans[u]], returned.at[g, spans[u]], bs.at[s, u], br.at[g, u], at(s, q)
            ))

    stages = {"F": spread, "G": relay, "C": compute, "M": reduce_mate, "E": reduce_pairs}
    plan = words(EXPERT_ORDER)
    lead = [word[:2] == "F0" for word in plan + [""]].index(False)
    dispatch(words(SEND_ORDER)[:3])
    for word in plan[:lead]:
        spread(0, int(word[2]))
    share()
    dispatch(words(SEND_ORDER)[3:])
    for word in plan[lead:]:
        stages[word[0]](int(word[1]), int(word[2]))
    for o in others:
        for u in range(subs):
            spot = returned.at[o, spans[u]]
            remote(spot, spot, bs.at[o, u], br.at[o, u], mate).wait_recv()


def layer_kernel(
    chips, groups, per_group, subs, chunks, *refs,
):
    inputs, outputs, scratch = refs[:21], refs[21:25], refs[25:]
    weights = inputs[18:]
    state, resid_ref, place_ref, returned = outputs
    rows_ref, shares_ref, picks, *rest = scratch
    front_scratch, rest = rest[:24], rest[24:]
    front_sems, rest = rest[:13], rest[13:]
    expert_scratch, expert_sems = rest[:12], rest[12:]
    loads = [
        pltpu.make_async_copy(src.at[0], dst, expert_sems[-1].at[i])
        for i, (src, dst) in enumerate(zip(weights, expert_scratch[7:10]))
    ]
    sends = []

    def meet(peers):
        grp = lax.axis_index("grp")
        me = lax.axis_index("ep")
        g, p = me // per_group, me % per_group
        ahead = [(grp, (g + i) % groups * per_group + p) for i in range(1, groups)]
        near = [(grp, g * per_group + (p + 2 * i) % per_group) for i in range(1, per_group // 2)]
        greet(peers + ahead + near)

    share_out = front(
        chips, per_group, sends, *inputs[:18], state, resid_ref, place_ref, rows_ref, shares_ref, picks,
        *front_scratch, *front_sems,
        meet, loads,
    )
    experts(
        groups, per_group, subs, chunks, sends, rows_ref, shares_ref, place_ref, returned,
        *expert_scratch, *expert_sems[:-1], loads,
        share_out,
    )
    for copy in sends:
        copy.wait_send()


def finish_kernel(state_ref, resid_ref, place_ref, returned_ref, new_any, out_any, out, sems, out_sem):
    count = sems.shape[1]
    step = state_ref.shape[1] // count
    copies = [
        pltpu.make_async_copy(
            state_ref.at[i, pl.ds(j * step, step)], new_any.at[i, pl.ds(j * step, step)], sems.at[i, j]
        )
        for i in range(2) for j in range(count)
    ]
    for copy in copies:
        copy.start()
    back = returned_ref[...].reshape(-1, returned_ref.shape[2])
    moe = jnp.dot(place_ref[...], back, preferred_element_type=F32)
    out[...] = (resid_ref[...].astype(F32) + moe).astype(BF16)
    copies.append(pltpu.make_async_copy(out, out_any, out_sem))
    copies[-1].start()
    for copy in copies:
        copy.wait()


def on_device(
    hidden, state, norm_gain, w_in, lam_re, lam_im, log_step, in_re, in_im, out_re, out_im, skip, w_glu, w_out,
    ffn_gain, w_group, w_route, w_gate, w_up, w_down, route_ids,
):
    rows, depth = hidden.shape
    devices = lax.axis_size("ep")
    chips = devices // 2
    shard = w_in.shape[1]
    dma = pltpu.SemaphoreType.DMA
    groups, entries = lam_re.shape
    width = in_re.shape[2]
    channels = groups * width
    lines = chips // 2
    blocks = channels // 128
    experts = w_route.shape[1]
    per_group = experts // EXP_GROUPS
    cap = 2 * rows // EXP_GROUPS
    pairs = per_group // 2
    G = EXP_GROUPS
    subs, chunks = 4, 2
    part, bulk = cap // subs, cap // chunks
    vm = pltpu.VMEM
    kept = [
        vm(state.shape, F32), vm((rows, depth), BF16), vm((rows, G * cap), BF16), vm((G, cap, depth), BF16),
    ]
    results = pl.pallas_call(
        functools.partial(layer_kernel, chips, G, per_group, subs, chunks),
        out_shape=kept,
        in_specs=[ANY] * 21,
        out_specs=[VMEM] * 4,
        scratch_shapes=[
            vm((rows, depth), BF16),
            vm((rows, 128), BF16),
            vm((rows, 128), jnp.int32),
            vm((chips, 2, shard, depth), BF16),
            vm((rows, depth), BF16),
        ] + [vm((channels, entries), F32)] * 4 + [
            vm(w_glu.shape, BF16),
            vm(w_out.shape, BF16),
            vm((rows, depth), BF16),
            vm((4, groups, 128), F32),
            vm((rows, channels), F32),
            vm((4, blocks, groups * entries // blocks // 128, 128), F32),
            vm((128, 2 * groups * entries // blocks), BF16),
            vm((128, 2 * groups * entries // blocks), BF16),
            vm((rows, 2 * groups * entries // blocks), BF16),
            vm((1, depth), F32), vm((groups, entries), F32), vm((groups, entries), F32), vm((1, groups), F32),
            vm((1, channels), F32), vm((1, depth), F32), vm((EXP_GROUPS, depth), BF16), vm((experts, depth), BF16),
            vm((TOPK, rows), jnp.int32),
        ] + [dma((lines, 4))] * 4 + [dma((chips, 2))] * 2 + [dma((chips, 6))] * 2
        + [dma((lines // 2, 4, lines // 2 - 1)), dma, dma, dma((17,)), dma((blocks,))] + [
            vm((G, cap, depth), BF16),
            vm((G, 2, pairs, cap, depth), BF16),
            vm((G, chunks, 2, pairs, bulk, depth), BF16),
            vm((G, chunks, pairs, bulk, depth), BF16),
            vm((G, subs, pairs, part, depth), BF16),
            vm((G, subs, pairs, part, depth), BF16),
            vm((G, cap, depth), BF16),
            vm(w_gate.shape[1:], BF16),
            vm(w_up.shape[1:], BF16),
            vm(w_down.shape[1:], BF16),
            vm((G * cap // 128, 8, 128), F32),
            vm((G, 2, pairs, 8, 128), F32),
        ] + [dma((G, subs))] * 2 + [dma((G, pairs, subs))] * 4 + [dma((G, chunks))] * 2 + [dma((G, pairs, subs))] * 2
        + [dma((G, subs))] * 2 + [dma((G,))] * 2 + [dma((G, pairs))] * 4 + [dma((3,))],
        compiler_params=pltpu.CompilerParams(collective_id=0, has_side_effects=True, vmem_limit_bytes=LIMIT),
        name="layer",
    )(
        hidden, norm_gain[None, :], w_in.T, state, lam_re, lam_im, log_step[None, :],
        in_re.transpose(0, 2, 1).reshape(channels, entries), in_im.transpose(0, 2, 1).reshape(channels, entries),
        out_re.reshape(channels, entries), out_im.reshape(channels, entries), skip[None, :], ffn_gain[None, :],
        w_glu, w_out, w_group.T, w_route.T, route_ids.T, w_gate, w_up, w_down,
    )
    new_state, hidden_out = pl.pallas_call(
        finish_kernel,
        out_shape=[jax.ShapeDtypeStruct(state.shape, F32), jax.ShapeDtypeStruct((rows, depth), BF16)],
        in_specs=[VMEM] * 4,
        out_specs=[ANY, ANY],
        scratch_shapes=[vm((rows, depth), BF16), dma((2, rows // 16)), dma],
        compiler_params=pltpu.CompilerParams(vmem_limit_bytes=FINISH_LIMIT),
        name="finish",
    )(*results)
    return (hidden_out, new_state)


def solution(mesh):
    return jax.shard_map(
        on_device,
        mesh=mesh,
        in_specs=(
            P(("grp", "ep"), None),
            P(None, ("grp", "ep"), None),
            P(),
            P(None, "ep"),
            P(),
            P(),
            P(),
            P(),
            P(),
            P(),
            P(),
            P(),
            P(),
            P(),
            P(),
            P(),
            P(),
            P("ep", None, None),
            P("ep", None, None),
            P("ep", None, None),
            P(("grp", "ep"), None),
        ),
        out_specs=(P(("grp", "ep"), None), P(None, ("grp", "ep"), None)),
        check_vma=False,
    )
```

```python
import functools

import jax
import jax.numpy as jnp
from jax import lax
from jax.experimental import pallas as pl
from jax.experimental.pallas import tpu as pltpu
from jax.sharding import PartitionSpec as P

EXP_GROUPS = 4
TOPK = 2
MESH = pl.DeviceIdType.MESH
VMEM = pl.BlockSpec(memory_space=pltpu.VMEM)
ANY = pl.BlockSpec(memory_space=pl.ANY)
F32 = jnp.float32
BF16 = jnp.bfloat16
NT = (((1,), (1,)), ((), ()))
TN = (((0,), (0,)), ((), ()))
GATHER_ORDER = (
    "p o0 a0 w", "o1 a1 b0 c0", "o4 o2 c1 b1", "A0 o5 a4 a2", "c2 a3 a5 o3", "A1 B0 b4 b2",
    "C0 am c3 C1", "c4 c5 om b5", "B1 b3 A2 cm", "A4 A3 A5 bm", "B4 C2 C4 B2", "C5 C3 Am B3",
    "B5 Cm Bm",
)
SEND_ORDER = (
    "30 11 20 10", "21 12 31 13", "22 32 23 33",
)
EXPERT_ORDER = (
    "F00 F02 F01 F03", "F11 G01 G00 F20", "G03 G02 F10 C00", "F21 F30 G20 C01", "F12 F31 G21 F13", "C20 F22 G30 G31",
    "G10 M20 M21 C30", "G11 F23 E20 G22", "F32 M31 C10 G23", "F33 M30 E21 C21", "M11 E31 G33 G32", "G13 M22 M10 E30",
    "C31 M23 M03 G12", "E11 E22 M33 C11", "M32 E23 E10 M12", "M13 M00 E33 M01", "E12 E32 M02 E13", "E02 E00 E01 E03",
)
LIMIT = 57 * 1024 * 1024
FINISH_LIMIT = 16 * 1024 * 1024


def remote(src, dst, send_sem, recv_sem, device):
    return pltpu.make_async_remote_copy(
        src_ref=src, dst_ref=dst, send_sem=send_sem, recv_sem=recv_sem, device_id=device, device_id_type=MESH
    )


def greet(peers):
    barrier = pltpu.get_barrier_semaphore()
    for peer in peers:
        pl.semaphore_signal(barrier, inc=1, device_id=peer, device_id_type=MESH)
    pl.semaphore_wait(barrier, len(peers))


def words(table):
    return [word for text in table for word in text.split()]


def front(
    chips, per_group, sends, hidden_any, gain_any, w_any, state_any, lam_re_any, lam_im_any, step_any, in_re_any, in_im_any,
    out_re_any, out_im_any, skip_any, ffn_gain_any, w_glu_any, w_out_any, w_group_any, w_route_any, ids_any,
    state, resid_ref, place_ref, rows_ref, shares_ref, picks,
    held, hidden, in_re, in_im, out_re, out_im, glu_w, out_w, normed, coef, active, strips, into, outof, rounded,
    gain_ref, lam_re_ref, lam_im_ref, step_ref, skip_ref, ffn_gain_ref, w_group_ref, w_route_ref, ids_ref,
    zs, zr, ys, yr, xs, xr, ds, dr, fs, own_s, own_r, load_sems, state_sems, meet, expert_loads,
):
    grp = lax.axis_index("grp")
    me = lax.axis_index("ep")
    chip, core = me // 2, me % 2
    lines = chips // 2
    line, y = chip // 2, chip % 2
    side = grp % 2
    shard, depth = w_any.shape
    entries = lam_re_any.shape[1]
    unit = 128 // (2 * shard)
    blocks = chips // unit
    span = state.shape[2] // blocks
    channels = 128 // (span // entries)

    def at(row, column):
        return (grp, (row * 2 + column) * 2 + core)

    mate = (grp, me + 1 - 2 * core)
    across = (grp + 1 - 2 * side, me)
    beside = at(line, 1 - y)
    half = lines // 2
    high = line // half
    low = high * half
    inside = [low + (line + i) % half for i in range(1, half)]
    crossing = [(half + i) * (1 - high) + (half - 1 - i) * high for i in range(half)]
    order = inside + crossing
    near_gate = (half - 1) * (1 - high) + half * high
    far_gate = half * (1 - high) + (half - 1) * high
    subs = 2
    part = shard // subs
    pieces = 2 * subs
    third = depth // 3 // 128 * 128
    middle = depth - 2 * third
    cols = [
        pl.ds(pl.multiple_of(side * (depth - third), 128), third),
        pl.ds(third, middle),
        pl.ds(pl.multiple_of((1 - side) * (depth - third), 128), third),
    ]

    def start(copy):
        copy.start()
        sends.append(copy)

    passed = []

    def view(chip_at, core_at, p):
        return held.at[chip_at, core_at, pl.ds(p % subs * part, part), cols[p // subs]]

    def column(j):
        return pl.ds(pl.multiple_of(j * span, span), span)

    own = pltpu.make_async_copy(w_any, held.at[chip, core], load_sems.at[0])
    own.start()
    loads = [
        pltpu.make_async_copy(src, dst, load_sems.at[1 + i])
        for i, (src, dst) in enumerate([
            (hidden_any, hidden), (in_re_any, in_re), (in_im_any, in_im), (out_re_any, out_re), (out_im_any, out_im),
            (w_glu_any, glu_w), (w_out_any, out_w), (gain_any, gain_ref), (lam_re_any, lam_re_ref), (lam_im_any, lam_im_ref),
            (step_any, step_ref), (skip_any, skip_ref), (ffn_gain_any, ffn_gain_ref), (w_group_any, w_group_ref),
            (w_route_any, w_route_ref), (ids_any, ids_ref),
        ])
    ]
    block_loads = [
        pltpu.make_async_copy(state_any.at[:, :, pl.ds(j * span, span)], state.at[:, :, pl.ds(j * span, span)], state_sems.at[j])
        for j in range(blocks)
    ]
    for load in loads[:1] + loads[7:] + loads[1:5] + block_loads + loads[5:7] + expert_loads:
        load.start()
    meet([at(o, y) for o in order] + [beside, mate, across])
    own.wait()
    for p in range(pieces):
        spot = view(chip, core, p)
        start(remote(spot, spot, ys.at[line, p], yr.at[line, p], beside))
        for o in inside + [far_gate]:
            start(remote(spot, spot, zs.at[o, p], zr.at[line, p], at(o, y)))
    spot = held.at[chip, core]
    start(remote(spot, spot, own_s, own_r, mate))

    def iota(shape, axis):
        return lax.broadcasted_iota(jnp.int32, shape, axis)

    def prepare():
        for load in loads[:5] + loads[7:] + block_loads:
            load.wait()
        prepare_all()

    tiles = span // 128
    stack = tiles * blocks

    def twin(value):
        return jnp.concatenate([value] * (128 // entries), axis=1)

    def prepare_all():
        wide = hidden[...].astype(F32)
        mean = jnp.mean(wide * wide, axis=-1, keepdims=True)
        normed[...] = (wide * lax.rsqrt(mean + 1e-06) * gain_ref[...]).astype(BF16)

        groups = lam_re_ref.shape[0]
        lr, li = lam_re_ref[...], lam_im_ref[...]
        diagonal = iota((groups, groups), 0) == iota((groups, groups), 1)
        step = jnp.exp(jnp.sum(jnp.where(diagonal, step_ref[...], 0.0), axis=1, keepdims=True))
        magnitude = jnp.exp(lr * step)
        bar_re = magnitude * jnp.cos(li * step)
        bar_im = magnitude * jnp.sin(li * step)
        denom = lr * lr + li * li
        lessened = bar_re - 1.0
        first_half = iota((stack, 128), 1) < entries
        for i, value in enumerate([
            bar_re, bar_im, (lessened * lr + bar_im * li) / denom, (bar_im * lr - lessened * li) / denom,
        ]):
            coef[i] = twin(value)
            even, odd = coef[i, pl.ds(0, stack, stride=2), :], coef[i, pl.ds(1, stack, stride=2), :]
            chosen = jnp.where(first_half, even, odd)
            for j in range(blocks):
                strips[i, j] = chosen[j * tiles : (j + 1) * tiles]
        into[...] = jnp.zeros_like(into)
        outof[...] = jnp.zeros_like(outof)

        count = hidden.shape[0]
        lane = iota((count, 128), 1)
        same = (iota((count, count), 0) == iota((count, count), 1)).astype(BF16)
        ids = lax.dot_general(same, ids_ref[...].astype(F32).astype(BF16), NT, preferred_element_type=F32).astype(jnp.int32)
        group = ids[:, 0:1] // per_group
        hits = (lane == group).astype(BF16)
        earlier = (iota((count, count), 1) < iota((count, count), 0)).astype(BF16)
        before = jnp.dot(earlier, hits, preferred_element_type=F32)
        rank = jnp.sum(jnp.where(lane == group, before, 0.0), axis=1, keepdims=True).astype(jnp.int32)
        slots = place_ref.shape[1]
        slot = group * (slots // EXP_GROUPS) + rank
        place_ref[...] = (iota((count, slots), 1) == slot).astype(BF16)
        picks[...] = jnp.where(lane == 0, ids[:, 0:1], ids[:, 1:2])

    rise = 128 // tiles
    inside_tile = iota((128, 128), 0) // channels % 2 == iota((128, 128), 1) // entries

    def expand(ref, j, target, base, sign):
        part_of = ref[pl.ds(pl.multiple_of(j * 128, 128), 128), :]
        tile = jnp.where(inside_tile, twin(part_of), 0.0)
        tile = (tile if sign > 0 else -tile).astype(BF16)
        for t in range(tiles):
            target[t * rise : (t + 1) * rise, base + t * 128 : base + (t + 1) * 128] = tile[t * rise : (t + 1) * rise]

    def mix(j):
        expand(in_re, j, into, 0, 1)
        expand(in_im, j, into, span, 1)
        expand(out_re, j, outof, 0, 1)
        expand(out_im, j, outof, span, -1)
        block = held[pl.ds(j * unit, unit)].reshape(128, depth)
        inputs = lax.dot_general(normed[...], block, NT, preferred_element_type=F32).astype(BF16)
        drive = jnp.dot(inputs, into[...], preferred_element_type=F32)
        strip = [strips[i, j] for i in range(4)]
        for t in range(tiles):
            lanes = pl.ds(pl.multiple_of(j * span + t * 128, 128), 128)
            row = [value[t : t + 1] for value in strip]
            drive_re = drive[:, t * 128 : (t + 1) * 128]
            drive_im = drive[:, span + t * 128 : span + (t + 1) * 128]
            old_re, old_im = state[0, :, lanes], state[1, :, lanes]
            new_re = row[0] * old_re - row[1] * old_im + (row[2] * drive_re - row[3] * drive_im)
            new_im = row[0] * old_im + row[1] * old_re + (row[2] * drive_im + row[3] * drive_re)
            state[0, :, lanes] = new_re
            state[1, :, lanes] = new_im
            rounded[:, t * 128 : (t + 1) * 128] = new_re.astype(BF16)
            rounded[:, span + t * 128 : span + (t + 1) * 128] = new_im.astype(BF16)
        read = lax.dot_general(rounded[...], outof[...], NT, preferred_element_type=F32)
        lanes = pl.ds(pl.multiple_of(j * 128, 128), 128)
        act = jax.nn.gelu(read + skip_ref[:, lanes] * inputs.astype(F32))
        active[:, lanes] = act

    def place(item):
        kind, k = item
        if kind == 0:
            return order[k] * 2 + y
        return (line if k < 0 else order[k]) * 2 + 1 - y

    def forward(k, p, spot):
        s = order[k]
        copies = [
            remote(spot, spot, fs.at[k - half + 1, p, i], zr.at[s, p], at(target, y)) for i, target in enumerate(inside)
        ]
        passed.extend(copies)

        @pl.when(line == near_gate)
        def _():
            for copy in copies:
                copy.start()

    def take(item, p):
        kind, k = item
        s = line if k < 0 else order[k]
        spot = view(place(item), core, p)
        if kind == 0:
            remote(spot, spot, zs.at[s, p], zr.at[s, p], mate).wait_recv()
            if k >= half - 1:
                forward(k, p, spot)
            start(remote(spot, spot, ys.at[s, p], yr.at[s, p], beside))
        else:
            remote(spot, spot, ys.at[s, p], yr.at[s, p], mate).wait_recv()
        if p < subs:
            start(remote(spot, spot, xs.at[place(item), p], xr.at[place(item), p], across))
        start(remote(spot, spot, ds.at[place(item), p], dr.at[place(item), p], mate))

    def take_x(item, u):
        spot = view(place(item), core, pieces + u)
        remote(spot, spot, xs.at[place(item), u], xr.at[place(item), u], mate).wait_recv()
        start(remote(spot, spot, ds.at[place(item), pieces + u], dr.at[place(item), pieces + u], mate))

    ready = {-1: 1}

    def finish(item):
        for p in range(pieces + subs):
            spot = view(place(item), 1 - core, p)
            remote(spot, spot, ds.at[place(item), p], dr.at[place(item), p], mate).wait_recv()
        if unit == 1:
            mix(place(item))
        else:
            k = item[1]
            ready[k] = ready.get(k, 0) + 1
            if ready[k] == unit:
                mix(line if k < 0 else order[k])

    names = {"o": (1, -1), "a": (0, 0), "b": (0, 1), "c": (0, 2), "A": (1, 0), "B": (1, 1), "C": (1, 2)}
    if lines == 4:
        plan = [(names.get(word[0]), word[-1]) for word in words(GATHER_ORDER)]
    else:
        items = [(1, -1)]
        for k in range(lines):
            if k < lines - 1:
                items.append((0, k))
            if k > 0:
                items.append((1, k - 1))
        plan = [(None, "p"), (None, "w")] + [(item, str(p)) for p in range(pieces) for item in items]
        plan += [(item, step) for item in items for step in [str(pieces + u) for u in range(subs)] + ["m"]]
    for item, step in plan:
        if step == "p":
            prepare()
        elif step == "w":
            spot = held.at[chip, 1 - core]
            remote(spot, spot, own_s, own_r, mate).wait_recv()
            if unit == 1:
                mix(chip)
        elif step == "m":
            finish(item)
        elif int(step) < pieces:
            take(item, int(step))
        else:
            take_x(item, int(step) - pieces)
    loads[5].wait()
    loads[6].wait()

    act = active[...]
    gating = jnp.dot(act.astype(BF16), glu_w[...], preferred_element_type=F32)
    glu = (act * jax.nn.sigmoid(gating)).astype(BF16)
    resid = (hidden[...].astype(F32) + jnp.dot(glu, out_w[...], preferred_element_type=F32)).astype(BF16)
    resid_ref[...] = resid
    wide = resid.astype(F32)
    mean = jnp.mean(wide * wide, axis=-1, keepdims=True)
    second_normed = (wide * lax.rsqrt(mean + 1e-06) * ffn_gain_ref[...]).astype(BF16)
    rows_ref[...] = second_normed

    def share_out():
        level = lax.dot_general(rows_ref[...], w_group_ref[...], NT, preferred_element_type=F32)
        logits = lax.dot_general(rows_ref[...], w_route_ref[...], NT, preferred_element_type=F32)
        first, second = picks[:, 0:1], picks[:, 1:2]
        lane = iota(picks.shape, 1)
        group = first // per_group
        chosen = jnp.sum(jnp.where(iota(level.shape, 1) == group, level, 0.0), axis=1, keepdims=True)
        scale = 1.0 / jnp.sum(jnp.exp(level - chosen), axis=1, keepdims=True)
        r0 = jnp.sum(jnp.where(iota(logits.shape, 1) == first, logits, 0.0), axis=1, keepdims=True)
        r1 = jnp.sum(jnp.where(iota(logits.shape, 1) == second, logits, 0.0), axis=1, keepdims=True)
        share = jax.nn.sigmoid(r0 - r1)
        member = lane % per_group
        gate = jnp.where(member == first % per_group, scale * share, 0.0)
        gate = gate + jnp.where(member == second % per_group, scale * (1.0 - share), 0.0)
        high = gate.astype(BF16).astype(F32)
        low_lanes = (lane >= 8) & (lane < 8 + per_group)
        shares_ref[...] = jnp.where(lane < per_group, high, jnp.where(low_lanes, gate - high, 0.0)).astype(BF16)
        return lax.dot_general(shares_ref[...], place_ref[...], TN, preferred_element_type=F32)

    @pl.when(line == near_gate)
    def _():
        for copy in passed:
            copy.wait_send()
    return share_out


def experts(
    groups, per_group, subs, chunks, sends, rows_ref, shares_ref, place_ref, returned,
    outgoing, tokens, parts, parts_in, sums, sums_in, final, w_gate, w_up, w_down, shares, shares_in,
    zs, zr, ys, yr, cs, cr, ps, pr, qs, qr, bs, br, gs, gr, hs, hr, ks, kr, loads, share_out,
):
    grp = lax.axis_index("grp")
    me = lax.axis_index("ep")
    pairs = per_group // 2
    g, p = me // per_group, me % per_group
    q, c = p // 2, p % 2
    depth = returned.shape[2]
    cap = outgoing.shape[1]
    wide = outgoing.shape[2]
    part = cap // subs
    spans = [pl.ds(i * part, part) for i in range(subs)]

    def at(group, pair):
        return (grp, group * per_group + pair * 2 + c)

    mate = (grp, me + 1 - 2 * c)
    half = groups // 2
    low = g // half * half
    crossing = [(low + half) % groups + (g + i) % half for i in range(half)]
    inside = [low + (g + i) % half for i in range(1, half)]
    sources = [g] + inside + crossing
    others = sources[1:]
    mates_q = [(q + j) % pairs for j in range(1, pairs)]
    sent = lax.dot_general(place_ref[...], rows_ref[...], TN, preferred_element_type=F32).astype(BF16)
    outgoing[...] = sent.reshape(groups, cap, wide)
    tokens[g, c, q] = outgoing[g]
    per_tile = 128 // cap

    def start(copy):
        copy.start()
        sends.append(copy)


    def share():
        split = share_out()
        joined = split[0:8] + split[8:16]
        for i in range(groups // per_tile):
            shares[i] = joined[:, i * 128 : (i + 1) * 128]
        shares_in[g, c, q] = shares[g // per_tile]
        for target in others:
            start(remote(shares.at[target // per_tile], shares_in.at[g, c, q], gs.at[target], gr.at[g], at(target, q)))
        pass_shares(0)

    def pass_shares(k):
        s = sources[k]
        spot = shares_in.at[s, c, q]
        if k > 0:
            remote(spot, spot, gs.at[s], gr.at[s], mate).wait_recv()
        for o in mates_q:
            start(remote(spot, spot, hs.at[s, o], hr.at[s, q], at(g, o)))
        start(remote(spot, spot, ks.at[s, q], kr.at[s, q], mate))

    def dispatch(plan):
        for word in plan:
            target, u = sources[int(word[0])], int(word[1])
            start(remote(
                outgoing.at[target, spans[u]], tokens.at[g, c, q, spans[u]], zs.at[target, u], zr.at[g, u], at(target, q)
            ))

    started = {"F": set(), "G": set(), "C": set()}

    def first_of(stage, k):
        fresh = k not in started[stage]
        started[stage].add(k)
        return fresh

    def spread(k, u):
        s = sources[k]
        if first_of("F", k) and k > 0:
            pass_shares(k)
        spot = tokens.at[s, c, q, spans[u]]
        if k > 0:
            remote(spot, spot, zs.at[s, u], zr.at[s, u], mate).wait_recv()
        for o in mates_q:
            start(remote(spot, spot, ys.at[s, o, u], yr.at[s, q, u], at(g, o)))
        start(remote(spot, spot, cs.at[s, q, u], cr.at[s, q, u], mate))

    def relay(k, u):
        s = sources[k]
        if first_of("G", k):
            for o in mates_q:
                spot = shares_in.at[s, c, o]
                remote(spot, spot, hs.at[s, o], hr.at[s, o], mate).wait_recv()
                start(remote(spot, spot, ks.at[s, o], kr.at[s, o], mate))
        for o in mates_q:
            spot = tokens.at[s, c, o, spans[u]]
            remote(spot, spot, ys.at[s, o, u], yr.at[s, o, u], mate).wait_recv()
            start(remote(spot, spot, cs.at[s, o, u], cr.at[s, o, u], mate))

    fold = subs // chunks
    bulk = cap // chunks

    def inner_rows(u):
        return pl.ds(u % fold * part, part)

    spread_rows = lax.broadcasted_iota(jnp.int32, (bulk, 128), 0)
    spread_lanes = lax.broadcasted_iota(jnp.int32, (bulk, 128), 1)

    def compute(k, h):
        s = sources[k]
        if first_of("C", k):
            for o in range(pairs):
                spot = shares_in.at[s, 1 - c, o]
                remote(spot, spot, ks.at[s, o], kr.at[s, o], mate).wait_recv()
        for u in range(h * fold, h * fold + fold):
            for o in range(pairs):
                spot = tokens.at[s, 1 - c, o, spans[u]]
                remote(spot, spot, cs.at[s, o, u], cr.at[s, o, u], mate).wait_recv()
        if not loaded:
            loaded.append(True)
            for load in loads:
                load.wait()
        total = per_group * bulk
        x = tokens[s, :, :, pl.ds(h * bulk, bulk)].reshape(total, wide)
        gate = jnp.dot(x, w_gate[...], preferred_element_type=F32)
        upper = jnp.dot(x, w_up[...], preferred_element_type=F32)
        inner = (jax.nn.silu(gate) * upper).astype(BF16)
        result = jnp.dot(inner, w_down[...], preferred_element_type=F32).astype(BF16)
        own_lane = spread_lanes == spread_rows + (g % per_tile * cap + h * bulk)
        weight = jnp.concatenate([
            jnp.sum(jnp.where(own_lane, shares_in[s, i, o, pl.ds(p, 1), :], 0.0), axis=1, keepdims=True)
            for i in range(2) for o in range(pairs)
        ], axis=0)
        parts[s, h] = (result.astype(F32) * weight).astype(BF16).reshape(2, pairs, bulk, depth)
        start(remote(parts.at[s, h, 1 - c], parts_in.at[s, h], ps.at[s, h], pr.at[s, h], mate))

    loaded = []
    merged = set()

    def reduce_mate(k, u):
        s, h = sources[k], u // fold
        if (k, h) not in merged:
            merged.add((k, h))
            spot = parts_in.at[s, h]
            remote(spot, spot, ps.at[s, h], pr.at[s, h], mate).wait_recv()
        sums[s, u] = (
            parts[s, h, c, :, inner_rows(u)].astype(F32) + parts_in[s, h, :, inner_rows(u)].astype(F32)
        ).astype(BF16)
        for o in mates_q:
            start(remote(sums.at[s, u, o], sums_in.at[s, u, q], qs.at[s, o, u], qr.at[s, q, u], at(g, o)))

    def reduce_pairs(k, u):
        s = sources[k]
        total = sums[s, u, q].astype(F32)
        for o in mates_q:
            spot = sums_in.at[s, u, o]
            remote(spot, spot, qs.at[s, o, u], qr.at[s, o, u], mate).wait_recv()
            total = total + sums_in[s, u, o].astype(F32)
        if k == 0:
            returned[g, spans[u]] = total.astype(BF16)
        else:
            final[s, spans[u]] = total.astype(BF16)
            start(remote(
                final.at[s, spans[u]], returned.at[g, spans[u]], bs.at[s, u], br.at[g, u], at(s, q)
            ))

    stages = {"F": spread, "G": relay, "C": compute, "M": reduce_mate, "E": reduce_pairs}
    plan = words(EXPERT_ORDER)
    lead = [word[:2] == "F0" for word in plan + [""]].index(False)
    dispatch(words(SEND_ORDER)[:1])
    for word in plan[:lead]:
        spread(0, int(word[2]))
    share()
    dispatch(words(SEND_ORDER)[1:])
    for word in plan[lead:]:
        stages[word[0]](int(word[1]), int(word[2]))
    for o in others:
        for u in range(subs):
            spot = returned.at[o, spans[u]]
            remote(spot, spot, bs.at[o, u], br.at[o, u], mate).wait_recv()


def layer_kernel(
    chips, groups, per_group, subs, chunks, *refs,
):
    inputs, outputs, scratch = refs[:21], refs[21:25], refs[25:]
    weights = inputs[18:]
    state, resid_ref, place_ref, returned = outputs
    rows_ref, shares_ref, picks, *rest = scratch
    front_scratch, rest = rest[:24], rest[24:]
    front_sems, rest = rest[:13], rest[13:]
    expert_scratch, expert_sems = rest[:12], rest[12:]
    loads = [
        pltpu.make_async_copy(src.at[0], dst, expert_sems[-1].at[i])
        for i, (src, dst) in enumerate(zip(weights, expert_scratch[7:10]))
    ]
    sends = []

    def meet(peers):
        grp = lax.axis_index("grp")
        me = lax.axis_index("ep")
        g, p = me // per_group, me % per_group
        ahead = [(grp, (g + i) % groups * per_group + p) for i in range(1, groups)]
        near = [(grp, g * per_group + (p + 2 * i) % per_group) for i in range(1, per_group // 2)]
        greet(peers + ahead + near)

    share_out = front(
        chips, per_group, sends, *inputs[:18], state, resid_ref, place_ref, rows_ref, shares_ref, picks,
        *front_scratch, *front_sems,
        meet, loads,
    )
    experts(
        groups, per_group, subs, chunks, sends, rows_ref, shares_ref, place_ref, returned,
        *expert_scratch, *expert_sems[:-1], loads,
        share_out,
    )
    for copy in sends:
        copy.wait_send()


def finish_kernel(state_ref, resid_ref, place_ref, returned_ref, new_any, out_any, out, sems, out_sem):
    count = sems.shape[1]
    step = state_ref.shape[1] // count
    copies = [
        pltpu.make_async_copy(
            state_ref.at[i, pl.ds(j * step, step)], new_any.at[i, pl.ds(j * step, step)], sems.at[i, j]
        )
        for i in range(2) for j in range(count)
    ]
    for copy in copies:
        copy.start()
    back = returned_ref[...].reshape(-1, returned_ref.shape[2])
    moe = jnp.dot(place_ref[...], back, preferred_element_type=F32)
    out[...] = (resid_ref[...].astype(F32) + moe).astype(BF16)
    copies.append(pltpu.make_async_copy(out, out_any, out_sem))
    copies[-1].start()
    for copy in copies:
        copy.wait()


def on_device(
    hidden, state, norm_gain, w_in, lam_re, lam_im, log_step, in_re, in_im, out_re, out_im, skip, w_glu, w_out,
    ffn_gain, w_group, w_route, w_gate, w_up, w_down, route_ids,
):
    rows, depth = hidden.shape
    devices = lax.axis_size("ep")
    chips = devices // 2
    shard = w_in.shape[1]
    dma = pltpu.SemaphoreType.DMA
    groups, entries = lam_re.shape
    width = in_re.shape[2]
    channels = groups * width
    lines = chips // 2
    blocks = channels // 128
    experts = w_route.shape[1]
    per_group = experts // EXP_GROUPS
    cap = 2 * rows // EXP_GROUPS
    pairs = per_group // 2
    G = EXP_GROUPS
    subs, chunks = 4, 2
    part, bulk = cap // subs, cap // chunks
    vm = pltpu.VMEM
    kept = [
        vm(state.shape, F32), vm((rows, depth), BF16), vm((rows, G * cap), BF16), vm((G, cap, depth), BF16),
    ]
    results = pl.pallas_call(
        functools.partial(layer_kernel, chips, G, per_group, subs, chunks),
        out_shape=kept,
        in_specs=[ANY] * 21,
        out_specs=[VMEM] * 4,
        scratch_shapes=[
            vm((rows, depth), BF16),
            vm((rows, 128), BF16),
            vm((rows, 128), jnp.int32),
            vm((chips, 2, shard, depth), BF16),
            vm((rows, depth), BF16),
        ] + [vm((channels, entries), F32)] * 4 + [
            vm(w_glu.shape, BF16),
            vm(w_out.shape, BF16),
            vm((rows, depth), BF16),
            vm((4, groups, 128), F32),
            vm((rows, channels), F32),
            vm((4, blocks, groups * entries // blocks // 128, 128), F32),
            vm((128, 2 * groups * entries // blocks), BF16),
            vm((128, 2 * groups * entries // blocks), BF16),
            vm((rows, 2 * groups * entries // blocks), BF16),
            vm((1, depth), F32), vm((groups, entries), F32), vm((groups, entries), F32), vm((1, groups), F32),
            vm((1, channels), F32), vm((1, depth), F32), vm((EXP_GROUPS, depth), BF16), vm((experts, depth), BF16),
            vm((TOPK, rows), jnp.int32),
        ] + [dma((lines, 4))] * 4 + [dma((chips, 2))] * 2 + [dma((chips, 6))] * 2
        + [dma((lines // 2, 4, lines // 2 - 1)), dma, dma, dma((17,)), dma((blocks,))] + [
            vm((G, cap, depth), BF16),
            vm((G, 2, pairs, cap, depth), BF16),
            vm((G, chunks, 2, pairs, bulk, depth), BF16),
            vm((G, chunks, pairs, bulk, depth), BF16),
            vm((G, subs, pairs, part, depth), BF16),
            vm((G, subs, pairs, part, depth), BF16),
            vm((G, cap, depth), BF16),
            vm(w_gate.shape[1:], BF16),
            vm(w_up.shape[1:], BF16),
            vm(w_down.shape[1:], BF16),
            vm((G * cap // 128, 8, 128), F32),
            vm((G, 2, pairs, 8, 128), F32),
        ] + [dma((G, subs))] * 2 + [dma((G, pairs, subs))] * 4 + [dma((G, chunks))] * 2 + [dma((G, pairs, subs))] * 2
        + [dma((G, subs))] * 2 + [dma((G,))] * 2 + [dma((G, pairs))] * 4 + [dma((3,))],
        compiler_params=pltpu.CompilerParams(collective_id=0, has_side_effects=True, vmem_limit_bytes=LIMIT),
        name="layer",
    )(
        hidden, norm_gain[None, :], w_in.T, state, lam_re, lam_im, log_step[None, :],
        in_re.transpose(0, 2, 1).reshape(channels, entries), in_im.transpose(0, 2, 1).reshape(channels, entries),
        out_re.reshape(channels, entries), out_im.reshape(channels, entries), skip[None, :], ffn_gain[None, :],
        w_glu, w_out, w_group.T, w_route.T, route_ids.T, w_gate, w_up, w_down,
    )
    new_state, hidden_out = pl.pallas_call(
        finish_kernel,
        out_shape=[jax.ShapeDtypeStruct(state.shape, F32), jax.ShapeDtypeStruct((rows, depth), BF16)],
        in_specs=[VMEM] * 4,
        out_specs=[ANY, ANY],
        scratch_shapes=[vm((rows, depth), BF16), dma((2, rows // 16)), dma],
        compiler_params=pltpu.CompilerParams(vmem_limit_bytes=FINISH_LIMIT),
        name="finish",
    )(*results)
    return (hidden_out, new_state)


def solution(mesh):
    return jax.shard_map(
        on_device,
        mesh=mesh,
        in_specs=(
            P(("grp", "ep"), None),
            P(None, ("grp", "ep"), None),
            P(),
            P(None, "ep"),
            P(),
            P(),
            P(),
            P(),
            P(),
            P(),
            P(),
            P(),
            P(),
            P(),
            P(),
            P(),
            P(),
            P("ep", None, None),
            P("ep", None, None),
            P("ep", None, None),
            P(("grp", "ep"), None),
        ),
        out_specs=(P(("grp", "ep"), None), P(None, ("grp", "ep"), None)),
        check_vma=False,
    )
```
